256 devices in a mesh: sp: 128 (over z, y, x), tp: 2 (over core).
Axes of the slice: x: 4, y: 4, z: 8, core: 2. Of those that a mesh axis runs over, the one named last changes fastest.
Arguments:
- queries: bfloat16 [196608, 1024], P('sp', 'tp'), may hold values from -6 to 6
- forget_logit: bfloat16 [196608, 1024], P('sp', 'tp'), may hold values from -8 to 8
- value_rows: bfloat16 [196608, 1024], P('sp', 'tp'), may hold values from -10 to 10
- out_gate: bfloat16 [196608, 1024], P('sp', 'tp'), may hold values from -6 to 6
- floor_gap: float32 [1024], P('tp'), may hold values from 0 to 0.1, as said below
- head_gain: float32 [1024], P('tp'), may hold values from 0.1 to 1.9
- state_in: float32 [8, 128, 128], P('tp'), may hold values from -0.625 to 0.625
- out_weight: bfloat16 [1024, 2048], P('tp'), may hold values from -0.1875 to 0.1875
Outputs:
- projected: bfloat16 [196608, 2048], P(('sp', 'tp'))
- state_out: float32 [8, 16384], P('tp', 'sp')
The draws below stay inside these ranges and needn't reach their ends.
Inputs may be any that keep to these rules, and one draw needn't show every extreme that they name: `floor_gap`: strictly between 0 and 0.1.
All inputs are finite; a program needn't handle non-finite values.
Results may differ from the reference program's by a relative error of at most 0.009.
Values may be sent and summed in bfloat16 or wider, within the bound.
No kernel may reach another device: no remote copies, remote signals or barrier semaphores. Data moves between devices by JAX's collectives and lax.ppermute only.
A program may use at most 128 MiB of HBM per device.

```python
import jax
import jax.numpy as jnp
from jax import lax

D = 2048
HEADS = 8
KEY_DIM = 128
VAL_DIM = 128
BLOCK = 128
SPAN = 1536
LENGTH = 196608
KEY_WIDTH = 1024
VAL_WIDTH = 1024


def stretch_offsets(key, width, scale):
    segment = max(SPAN // 2, 1)
    count = LENGTH // segment
    offsets = scale * jax.random.normal(key, (count, 1, width), jnp.float32)
    return jnp.broadcast_to(offsets, (count, segment, width)).reshape(LENGTH, width)


def draw_forget_logit(key, part):
    noise_key, shift_key = jax.random.split(jax.random.fold_in(key, 11))
    noise = jnp.clip(jax.random.normal(noise_key, (LENGTH, KEY_WIDTH), jnp.float32), -4.0, 4.0)
    shift = jnp.clip(stretch_offsets(shift_key, KEY_WIDTH, 1.5), -4.0, 4.0)
    return (noise + shift).astype(jnp.bfloat16)


def draw_value_rows(key, part):
    noise_key, shift_key = jax.random.split(jax.random.fold_in(key, 13))
    noise = jnp.clip(jax.random.normal(noise_key, (LENGTH, VAL_WIDTH), jnp.float32), -4.0, 4.0)
    shift = jnp.clip(stretch_offsets(shift_key, VAL_WIDTH, 2.0), -6.0, 6.0)
    return (noise + shift).astype(jnp.bfloat16)


def draw_floor_gap(key, part):
    ranking_key, slow_key, fast_key = jax.random.split(jax.random.fold_in(key, 5), 3)
    ranking = jax.random.permutation(ranking_key, HEADS)
    fast_count = HEADS // 2
    fast_head = jnp.repeat(ranking < fast_count, KEY_DIM)
    slow_gap = jnp.exp(jax.random.uniform(slow_key, (KEY_WIDTH,), jnp.float32, jnp.log(0.5), jnp.log(2.0))) / LENGTH
    fast_gap = jnp.exp(jax.random.uniform(fast_key, (KEY_WIDTH,), jnp.float32, jnp.log(0.03), jnp.log(0.08)))
    return jnp.where(fast_head, fast_gap, slow_gap)


def levels(rng, dims, cuts, smallest, top_value):
    factor_of, own = 1.0, jax.random.fold_in(rng, 6)
    for axis_at, blocks in cuts:
        draws = jnp.exp(jax.random.uniform(jax.random.fold_in(own, axis_at), (blocks,), jnp.float32, smallest / len(cuts), top_value / len(cuts)))
        factor_of = factor_of * jnp.repeat(draws, dims[axis_at] // blocks).reshape([-1 if axis == axis_at else 1 for axis in range(len(dims))])
    return factor_of


def normal_values(key, dims, scale, most, cuts=(), dtype=jnp.bfloat16):
    level = levels(key, dims, cuts, -0.22, 0.18) if cuts else 1.0
    entries = jax.random.normal(key, dims, jnp.float32) * scale * level
    return jnp.minimum(jnp.maximum(entries, -most), most).astype(dtype)


def setup_inputs(seed: int = 0) -> dict:
    splits = jax.random.split(jax.random.key(seed), 9)
    return {
        "queries": normal_values(splits[0], (LENGTH, KEY_WIDTH), 1.0, 6.0, ((0, 128), (1, 2))),
        "forget_logit": draw_forget_logit(jax.random.fold_in(splits[8], 71), 0),
        "value_rows": draw_value_rows(jax.random.fold_in(splits[8], 71), 0),
        "out_gate": normal_values(splits[3], (LENGTH, VAL_WIDTH), 1.0, 6.0, ((0, 128), (1, 2))),
        "floor_gap": draw_floor_gap(jax.random.fold_in(splits[8], 71), 0),
        "head_gain": jnp.clip(1.0 + 0.18 * jax.random.normal(splits[5], (VAL_WIDTH,), jnp.float32), 0.1, 1.9),
        "state_in": normal_values(splits[6], (HEADS, KEY_DIM, VAL_DIM), 0.1, 0.625, ((0, 2),), jnp.float32),
        "out_weight": normal_values(splits[7], (VAL_WIDTH, D), VAL_WIDTH ** -0.5, 0.1875, ((0, 2),)),
    }


maximum_precision = lax.Precision.HIGHEST
epsilon = 1e-06

def reference(queries, forget_logit, value_rows, out_gate, floor_gap, head_gain, state_in, out_weight):
    blocks = LENGTH // BLOCK
    gap_rows = floor_gap.reshape(HEADS, KEY_DIM)
    gain_rows = head_gain.reshape(HEADS, VAL_DIM)
    causal = jnp.arange(BLOCK)[:, None] >= jnp.arange(BLOCK)[None, :]

    def to_heads(values, width):
        return values.reshape(blocks, BLOCK, HEADS, width).transpose(0, 2, 1, 3)
    inputs = (to_heads(queries, KEY_DIM), to_heads(forget_logit, KEY_DIM), to_heads(value_rows, VAL_DIM), to_heads(out_gate, VAL_DIM))

    def advance(passed_forward, pieces):
        query_block, logit_block, value_block, gate_block = pieces
        key_gate = gap_rows[:, None, :] * jax.nn.sigmoid(-logit_block.astype(jnp.float32))
        log_forget = jnp.log1p(-key_gate)
        reader = jax.nn.silu(query_block.astype(jnp.float32))
        written_update = value_block.astype(jnp.float32)
        cumul = jnp.cumsum(log_forget, axis=1)
        scaled_readout = reader * jnp.exp(cumul)
        scores = jnp.einsum('hck,hsk->hcs', scaled_readout, key_gate * jnp.exp(-cumul), precision=maximum_precision)
        scores = jnp.where(causal[None], scores, 0.0)
        unscaled_output = jnp.einsum('hcs,hsv->hcv', scores, written_update, precision=maximum_precision)
        unscaled_output = unscaled_output + jnp.einsum('ufx,uxa->ufa', scaled_readout, passed_forward, precision=maximum_precision)
        block_log_decay = cumul[:, -1]
        decay_to_finish = key_gate * jnp.exp(block_log_decay[:, None, :] - cumul)
        refreshed_state = jnp.exp(block_log_decay)[..., None] * passed_forward + jnp.einsum('lxr,lxf->lrf', decay_to_finish, written_update, precision=maximum_precision)
        mean_square = lax.optimization_barrier(jnp.mean(unscaled_output * unscaled_output, axis=-1, keepdims=True))
        normed = unscaled_output * lax.rsqrt(mean_square + epsilon) * gain_rows[:, None, :]
        gated = (normed * jax.nn.silu(gate_block.astype(jnp.float32))).astype(jnp.bfloat16)
        return (refreshed_state, gated)
    state_out, gated = lax.scan(advance, state_in, inputs)
    gated = gated.transpose(0, 2, 1, 3).reshape(LENGTH, VAL_WIDTH)
    projected = jnp.dot(gated, out_weight, preferred_element_type=jnp.float32).astype(jnp.bfloat16)
    return (projected, state_out.reshape(HEADS, KEY_DIM * VAL_DIM))
```

```python
import functools

import jax
import jax.numpy as jnp
from jax import lax
from jax.experimental import pallas as pl
from jax.experimental.pallas import tpu as pltpu
from jax.sharding import Mesh
from jax.sharding import PartitionSpec as P

BLOCK = 128
EPSILON = 1e-06
Z, Y, X = ("sp_0", "sp_1", "sp_2")
SP = (Z, Y, X)
PLANE = (Y, X)
SP_TP = (Z, Y, X, "tp")
F32 = jnp.float32
BF16 = jnp.bfloat16


def mm(a, b, dims=((1,), (0,))):
    return lax.dot_general(a, b, (dims, ((), ())), preferred_element_type=F32)


def iota(shape, axis):
    return lax.broadcasted_iota(jnp.int32, shape, axis)


def params(limit_mib):
    return pltpu.CompilerParams(
        dimension_semantics=("arbitrary",), vmem_limit_bytes=limit_mib * 1024 * 1024
    )


def deal_matrix(plane, depth, transposed):
    rows = plane * depth
    dealt = iota((rows, rows), 1 if transposed else 0)
    natural = iota((rows, rows), 0 if transposed else 1)
    return ((dealt % depth) * plane + dealt // depth == natural).astype(BF16)


def state_kernel(heads, plane, depth, gap, logit, value, key_out, grow_out, start_out, offset_out,
                 send_out, state, decay, pair):
    step = pl.program_id(0)

    @pl.when(step == 0)
    def _():
        state[...] = jnp.zeros_like(state)
        decay[...] = jnp.ones_like(decay)

    lower = (iota((BLOCK, BLOCK), 0) >= iota((BLOCK, BLOCK), 1)).astype(BF16)
    lower2 = jnp.concatenate([lower, lower], axis=1)
    for b in range(logit.shape[0] // BLOCK):
        rows = pl.ds(b * BLOCK, BLOCK)
        key_gate = gap[...] * jax.nn.sigmoid(-logit[rows, :].astype(F32))
        log_forget = jnp.log1p(-key_gate)
        high = log_forget.astype(BF16)
        low = (log_forget - high.astype(F32)).astype(BF16)
        cumul = mm(lower2, jnp.concatenate([high, low], axis=0))
        grow = jnp.exp(cumul)
        key = (key_gate * jnp.exp(-cumul)).astype(BF16)
        grow_out[rows, :] = grow
        key_out[rows, :] = key
        start_out[b] = state[...].astype(BF16)
        offset_out[b] = decay[...]
        block_decay = grow[BLOCK - 1 :, :]
        for h in range(heads):
            cols = pl.ds(h * 128, 128)
            update = mm(value[rows, cols], key[:, h * 128 : (h + 1) * 128], ((0,), (0,)))
            state[:, cols] = block_decay[:, h * 128 : (h + 1) * 128] * (state[:, cols] + update)
        decay[...] = decay[...] * block_decay

    @pl.when(step == pl.num_programs(0) - 1)
    def _():
        deal = deal_matrix(plane, depth, False)
        for h in range(heads):
            cols = pl.ds(h * 128, 128)
            dealt = mm(deal, state[:, cols].astype(BF16), ((1,), (1,)))
            send_out[:, h * depth : (h + 1) * depth, :] = (
                dealt.reshape(plane, depth, 128).astype(BF16)
            )
            whole = decay[:, cols]
            high = whole.astype(BF16).astype(F32)
            pair[h : h + 1, :] = high
            pair[heads + h : heads + h + 1, :] = whole - high
        tail = pair[...].astype(BF16)
        for p in range(plane):
            send_out[p, heads * depth :, :] = tail


def local_state(gap, logit, value, heads, plane, depth, rows):
    span, width = logit.shape
    blocks = rows // BLOCK
    tall = pl.BlockSpec((rows, width), lambda i: (i, 0))
    whole = pl.BlockSpec((1, width), lambda i: (0, 0))
    sent = (plane, heads * depth + 2 * heads, 128)
    return pl.pallas_call(
        functools.partial(state_kernel, heads, plane, depth),
        grid=(span // rows,),
        in_specs=[whole, tall, tall],
        out_specs=[
            tall,
            tall,
            pl.BlockSpec((blocks, 128, width), lambda i: (i, 0, 0)),
            pl.BlockSpec((blocks, 1, width), lambda i: (i, 0, 0)),
            pl.BlockSpec(sent, lambda i: (0, 0, 0)),
        ],
        out_shape=[
            jax.ShapeDtypeStruct((span, width), BF16),
            jax.ShapeDtypeStruct((span, width), F32),
            jax.ShapeDtypeStruct((span // BLOCK, 128, width), BF16),
            jax.ShapeDtypeStruct((span // BLOCK, 1, width), F32),
            jax.ShapeDtypeStruct(sent, BF16),
        ],
        scratch_shapes=[
            pltpu.VMEM((128, width), F32),
            pltpu.VMEM((1, width), F32),
            pltpu.VMEM((2 * heads, 128), F32),
        ],
        compiler_params=params(24),
        cost_estimate=pl.CostEstimate(flops=6_000_000_000, bytes_accessed=10_000_000, transcendentals=0),
        name="stretch_state",
    )(gap, logit, value)


def output_kernel(heads, which, query, key, grow, value, start, offset, gate, gain,
                  raw_out, reach_out, gated_out):
    causal = iota((BLOCK, BLOCK), 0) >= iota((BLOCK, BLOCK), 1)
    for b in range(query.shape[0] // BLOCK):
        rows = pl.ds(b * BLOCK, BLOCK)
        for h in range(heads):
            cols = pl.ds(h * 128, 128)
            reader = jax.nn.silu(query[rows, cols].astype(F32)) * grow[rows, cols]
            reader_low = reader.astype(BF16)
            reach_out[rows, cols] = (reader * offset[b][:, h * 128 : (h + 1) * 128]).astype(BF16)
            scores = mm(reader_low, key[rows, cols], ((1,), (1,)))
            scores = jnp.where(causal, scores, 0.0).astype(BF16)
            raw_out[rows, cols] = mm(scores, value[rows, cols]) + mm(
                reader_low, start[b, :, cols], ((1,), (1,))
            )
            gated_out[rows, cols] = jax.nn.silu(gate[rows, cols].astype(F32)) * gain[:, cols]


def local_output(which, query, key, grow, value, start, offset, gate, gain, heads, rows):
    span, width = query.shape
    half = span // 2
    steps = half // rows
    blocks = rows // BLOCK
    read = pl.BlockSpec((rows, width), lambda i, w: (w[0] * steps + i, 0))
    write = pl.BlockSpec((rows, width), lambda i, w: (i, 0))
    return pl.pallas_call(
        functools.partial(output_kernel, heads),
        grid_spec=pltpu.PrefetchScalarGridSpec(
            num_scalar_prefetch=1,
            grid=(steps,),
            in_specs=[
                read,
                read,
                read,
                read,
                pl.BlockSpec((blocks, 128, width), lambda i, w: (w[0] * steps + i, 0, 0)),
                pl.BlockSpec((blocks, 1, width), lambda i, w: (w[0] * steps + i, 0, 0)),
                read,
                pl.BlockSpec((1, width), lambda i, w: (0, 0)),
            ],
            out_specs=[write, write, write],
        ),
        out_shape=[
            jax.ShapeDtypeStruct((half, width), F32),
            jax.ShapeDtypeStruct((half, width), BF16),
            jax.ShapeDtypeStruct((half, width), F32),
        ],
        compiler_params=params(24),
        cost_estimate=pl.CostEstimate(flops=6_000_000_000, bytes_accessed=10_000_000, transcendentals=0),
        name="stretch_output",
    )(which, query, key, grow, value, start, offset, gate, gain)


def decay_columns(place, received, heads, depth, plane):
    count = received.shape[0]
    picked = (iota((depth, 128), 1) == iota((depth, 128), 0) * plane + place).astype(BF16)
    parts = received[:, heads * depth :, :].reshape(count * 2 * heads, 128)
    columns = mm(picked, parts, ((1,), (1,)))
    lanes = columns.shape[1]
    return columns + pltpu.roll(columns, lanes - heads, 1)


def plane_kernel(heads, plane, depth, place, received, send_out, prefix_out, product_out):
    columns = decay_columns(place[0], received, heads, depth, plane)
    total = None
    states = [jnp.zeros((depth, 128), F32) for _ in range(heads)]
    products = [jnp.ones((depth, 128), F32) for _ in range(heads)]
    for s in range(plane):
        parts = received[s, heads * depth :, :].astype(F32)
        row_decay = parts + pltpu.roll(parts, heads, 0)
        total = row_decay if total is None else total * row_decay
        for h in range(heads):
            rows = slice(h * depth, (h + 1) * depth)
            prefix_out[s, rows, :] = states[h]
            product_out[s, rows, :] = products[h]
            lane = s * 2 * heads + h
            decay = jnp.broadcast_to(columns[:, lane : lane + 1], (depth, 128))
            states[h] = decay * states[h] + received[s, rows, :].astype(F32)
            products[h] = decay * products[h]
    high = total.astype(BF16).astype(F32)
    tail = jnp.where(iota(total.shape, 0) < heads, high, total - high).astype(BF16)
    for d in range(send_out.shape[0]):
        for h in range(heads):
            send_out[d, h * depth : (h + 1) * depth, :] = states[h].astype(BF16)
        send_out[d, heads * depth :, :] = tail


def plane_scan(place, received, heads, depth):
    plane, tall, _ = received.shape
    rows = heads * depth
    return pl.pallas_call(
        functools.partial(plane_kernel, heads, plane, depth),
        grid_spec=pltpu.PrefetchScalarGridSpec(
            num_scalar_prefetch=1,
            grid=(1,),
            in_specs=[pl.BlockSpec((plane, tall, 128), lambda i, w: (0, 0, 0))],
            out_specs=[
                pl.BlockSpec((depth, tall, 128), lambda i, w: (0, 0, 0)),
                pl.BlockSpec((plane, rows, 128), lambda i, w: (0, 0, 0)),
                pl.BlockSpec((plane, rows, 128), lambda i, w: (0, 0, 0)),
            ],
        ),
        out_shape=[
            jax.ShapeDtypeStruct((depth, tall, 128), BF16),
            jax.ShapeDtypeStruct((plane, rows, 128), F32),
            jax.ShapeDtypeStruct((plane, rows, 128), F32),
        ],
        compiler_params=params(8),
        cost_estimate=pl.CostEstimate(flops=100_000_000, bytes_accessed=1_000_000, transcendentals=0),
        name="plane_scan",
    )(place, received)


def depth_kernel(heads, plane, depth, place, received, prefix, product, first, send_out, final_out,
                 entering, final):
    columns = decay_columns(place[0], received, heads, depth, plane)
    states = [first[h] for h in range(heads)]
    for s in range(depth):
        for h in range(heads):
            rows = slice(h * depth, (h + 1) * depth)
            entering[s, rows, :] = states[h]
            lane = s * 2 * heads + h
            decay = jnp.broadcast_to(columns[:, lane : lane + 1], (depth, 128))
            states[h] = decay * states[h] + received[s, rows, :].astype(F32)
    for h in range(heads):
        final[h] = states[h]
        final_out[h : h + 1, :] = final[h, pl.ds(place[1], 1), :]
    mine = entering[place[1]]
    for p in range(plane):
        send_out[p] = (prefix[p] + product[p] * mine).astype(BF16)


def depth_scan(place, received, prefix, product, first, heads):
    depth, tall, _ = received.shape
    plane, rows, _ = prefix.shape
    return pl.pallas_call(
        functools.partial(depth_kernel, heads, plane, depth),
        grid_spec=pltpu.PrefetchScalarGridSpec(
            num_scalar_prefetch=1,
            grid=(1,),
            in_specs=[
                pl.BlockSpec((depth, tall, 128), lambda i, w: (0, 0, 0)),
                pl.BlockSpec((plane, rows, 128), lambda i, w: (0, 0, 0)),
                pl.BlockSpec((plane, rows, 128), lambda i, w: (0, 0, 0)),
                pl.BlockSpec((heads, depth, 128), lambda i, w: (0, 0, 0)),
            ],
            out_specs=[
                pl.BlockSpec((plane, rows, 128), lambda i, w: (0, 0, 0)),
                pl.BlockSpec((heads, 128), lambda i, w: (0, 0)),
            ],
            scratch_shapes=[
                pltpu.VMEM((depth, rows, 128), F32),
                pltpu.VMEM((heads, depth, 128), F32),
            ],
        ),
        out_shape=[
            jax.ShapeDtypeStruct((plane, rows, 128), BF16),
            jax.ShapeDtypeStruct((heads, 128), F32),
        ],
        compiler_params=params(8),
        cost_estimate=pl.CostEstimate(flops=100_000_000, bytes_accessed=1_000_000, transcendentals=0),
        name="depth_scan",
    )(place, received, prefix, product, first)


def finish_kernel(heads, depth, incoming, raw, reach, gating, gated_out, state):
    plane = incoming.shape[0]

    @pl.when(pl.program_id(0) == 0)
    def _():
        collect = deal_matrix(plane, depth, True)
        for h in range(heads):
            part = incoming[:, h * depth : (h + 1) * depth, :].astype(F32)
            part = part.reshape(plane * depth, 128).astype(BF16)
            state[h] = mm(collect, part).astype(BF16)

    mean = jnp.full((128, 128), 1.0 / 128, BF16)
    for b in range(raw.shape[0] // BLOCK):
        rows = pl.ds(b * BLOCK, BLOCK)
        for h in range(heads):
            cols = pl.ds(h * 128, 128)
            value = raw[rows, cols] + mm(reach[rows, cols], state[h])
            mean_square = mm((value * value).astype(BF16), mean)
            gated_out[rows, cols] = (
                value * lax.rsqrt(mean_square + EPSILON) * gating[rows, cols]
            ).astype(BF16)


def finish(incoming, raw, reach, gating, heads, depth, rows):
    span, width = raw.shape
    tall = pl.BlockSpec((rows, width), lambda i: (i, 0))
    return pl.pallas_call(
        functools.partial(finish_kernel, heads, depth),
        grid=(span // rows,),
        in_specs=[pl.BlockSpec(incoming.shape, lambda i: (0, 0, 0)), tall, tall, tall],
        out_specs=tall,
        out_shape=jax.ShapeDtypeStruct((span, width), BF16),
        scratch_shapes=[pltpu.VMEM((heads, 128, 128), BF16)],
        compiler_params=params(16),
        cost_estimate=pl.CostEstimate(flops=2_000_000_000, bytes_accessed=4_000_000, transcendentals=0),
        name="finish",
    )(incoming, raw, reach, gating)


def project_kernel(mine, theirs, my_weight, their_weight, out):
    total = mm(mine[...], my_weight[...]) + mm(theirs[...], their_weight[...])
    out[...] = total.astype(BF16)


def project(mine, theirs, my_weight, their_weight, cols):
    rows, inner = mine.shape
    width = my_weight.shape[1]
    left = pl.BlockSpec((rows, inner), lambda i: (0, 0))
    right = pl.BlockSpec((inner, cols), lambda i: (0, i))
    return pl.pallas_call(
        project_kernel,
        grid=(width // cols,),
        in_specs=[left, left, right, right],
        out_specs=pl.BlockSpec((rows, cols), lambda i: (0, i)),
        out_shape=jax.ShapeDtypeStruct((rows, width), BF16),
        compiler_params=params(24),
        cost_estimate=pl.CostEstimate(flops=3_300_000_000, bytes_accessed=9_000_000, transcendentals=0),
        name="project",
    )(mine, theirs, my_weight, their_weight)


def per_device(
    queries, forget_logit, value_rows, out_gate, floor_gap, head_gain, state_in, out_weight
):
    heads = state_in.shape[0]
    plane = lax.axis_size(PLANE)
    depth = lax.axis_size(Z)
    place_plane = lax.axis_index(PLANE)
    place = jnp.stack([place_plane, lax.axis_index(Z)]).astype(jnp.int32)
    core = lax.axis_index("tp")
    other_half = (1 - core).reshape(1).astype(jnp.int32)
    my_half = core.reshape(1).astype(jnp.int32)
    swap = [(0, 1), (1, 0)]
    barrier = lax.optimization_barrier

    their_weight = lax.ppermute(out_weight, "tp", swap)
    gap = floor_gap.reshape(1, -1)
    gain = head_gain.reshape(1, -1)
    first = lax.dynamic_index_in_dim(
        state_in.reshape(heads, depth, plane, 128), place_plane, 2, keepdims=False
    )

    key, grow, start, offset, send = local_state(
        gap, forget_logit, value_rows, heads, plane, depth, 384
    )
    received = lax.all_to_all(send, PLANE, 0, 0, tiled=True)
    far = local_output(
        other_half, queries, key, grow, value_rows, start, offset, out_gate, gain, heads, 384
    )
    received, far, key = barrier((received, far, key))

    send, prefix, product = plane_scan(place, received, heads, depth)
    received = lax.all_to_all(send, Z, 0, 0, tiled=True)
    near = local_output(
        my_half, queries, key, grow, value_rows, start, offset, out_gate, gain, heads, 384
    )
    received, near = barrier((received, near))

    send, state_out = depth_scan(place, received, prefix, product, first, heads)
    incoming = lax.all_to_all(send, PLANE, 0, 0, tiled=True)

    far_gated = finish(incoming, *far, heads, depth, 384)
    theirs = lax.ppermute(far_gated, "tp", swap)
    mine = finish(incoming, *near, heads, depth, 384)
    projected = project(mine, theirs, out_weight, their_weight, 256)
    return (projected, state_out)


def solution(mesh):
    torus = Mesh(mesh.devices.reshape(8, 4, 4, mesh.shape["tp"]), (Z, Y, X, "tp"))
    placed = (
        P(SP, "tp"),
        P(SP, "tp"),
        P(SP, "tp"),
        P(SP, "tp"),
        P("tp"),
        P("tp"),
        P("tp", None, None),
        P("tp", None),
    )
    return jax.shard_map(
        per_device,
        mesh=torus,
        in_specs=placed,
        out_specs=(P(SP_TP, None), P("tp", SP)),
        check_vma=False,
    )
```

```python
import functools

import jax
import jax.numpy as jnp
from jax import lax
from jax.experimental import pallas as pl
from jax.experimental.pallas import tpu as pltpu
from jax.sharding import Mesh
from jax.sharding import PartitionSpec as P

BLOCK = 128
UNROLL = 3
EPSILON = 1e-06
LOG2E = 1.4426950408889634
Z, Y, X = ("sp_0", "sp_1", "sp_2")
SP = (Z, Y, X)
PLANE = (Y, X)
SP_TP = (Z, Y, X, "tp")
F32 = jnp.float32
BF16 = jnp.bfloat16


def mm(a, b, dims=((1,), (0,))):
    return lax.dot_general(a, b, (dims, ((), ())), preferred_element_type=F32)


def iota(shape, axis):
    return lax.broadcasted_iota(jnp.int32, shape, axis)


def params(limit_mib):
    return pltpu.CompilerParams(
        dimension_semantics=("arbitrary",), vmem_limit_bytes=limit_mib * 1024 * 1024
    )


def deal_matrix(plane, depth, transposed):
    rows = plane * depth
    dealt = iota((rows, rows), 1 if transposed else 0)
    natural = iota((rows, rows), 0 if transposed else 1)
    return ((dealt % depth) * plane + dealt // depth == natural).astype(BF16)


def log2_of_rest(gate):
    near = gate * (gate * (gate * (-LOG2E / 3) - LOG2E / 2) - LOG2E)
    return jnp.where(gate < 1e-3, near, jnp.log2(1.0 - gate))


def stretch_kernel(heads, plane, depth, unroll, gap_in, gain_in, query_in, logit_in, value_in,
                   gate_in, raw_out, reach_out, gating_out, send_out,
                   query, logit, value, gate, key_gates, cumuls, gap, gain, state, decay, pair, sems, small_sems):
    blocks = query.shape[0] // BLOCK
    sides = ((logit_in, logit), (value_in, value), (query_in, query), (gate_in, gate))

    def copies(i, first, last):
        rows = pl.ds(i * unroll * BLOCK, unroll * BLOCK)
        return [
            pltpu.make_async_copy(source.at[rows, :], target.at[rows, :], sems.at[n, i])
            for n, (source, target) in list(enumerate(sides))[first:last]
        ]

    small = [
        pltpu.make_async_copy(gap_in, gap, small_sems.at[0]),
        pltpu.make_async_copy(gain_in, gain, small_sems.at[1]),
    ]
    for copy in small:
        copy.start()
    for part in ((0, 1), (1, 4)):
        for i in range(blocks // unroll):
            for copy in copies(i, *part):
                copy.start()
    state[...] = jnp.zeros_like(state)
    decay[...] = jnp.ones_like(decay)
    causal = iota((BLOCK, BLOCK), 0) >= iota((BLOCK, BLOCK), 1)
    lower = causal.astype(BF16)
    lower2 = jnp.concatenate([lower, lower], axis=1)
    head_cols = [pl.ds(h * 128, 128) for h in range(heads)]
    for copy in small:
        copy.wait()

    def rows_of(block):
        return pl.ds(pl.multiple_of(block * BLOCK, BLOCK), BLOCK)

    def sum_logs(i, carry):
        for copy in copies(i, 0, 1):
            copy.wait()
        for b in range(unroll):
            rows = rows_of(i * unroll + b)
            highs, lows = [], []
            for cols in head_cols:
                key_gate = gap[:, cols] * jax.nn.sigmoid(-logit[rows, cols].astype(F32))
                key_gates[rows, cols] = key_gate
                log_forget = log2_of_rest(key_gate)
                highs.append(log_forget.astype(BF16))
                lows.append((log_forget - highs[-1].astype(F32)).astype(BF16))
            split = jnp.concatenate(
                [jnp.concatenate(highs, axis=1), jnp.concatenate(lows, axis=1)], axis=0
            )
            cumuls[rows, :] = mm(lower2, split)
        return carry

    lax.fori_loop(0, blocks // unroll, sum_logs, 0)

    def advance(i, carry):
        for copy in copies(i, 1, 4):
            copy.wait()
        for b in range(unroll):
            rows = rows_of(i * unroll + b)
            scores, inters, updates, decays = [], [], [], []
            for cols in head_cols:
                cumul = cumuls[rows, cols]
                grow = jnp.exp2(cumul)
                key = (key_gates[rows, cols] * jnp.exp2(-cumul)).astype(BF16)
                reader = jax.nn.silu(query[rows, cols].astype(F32)) * grow
                reach_out[rows, cols] = (reader * decay[:, cols]).astype(BF16)
                reader = reader.astype(BF16)
                scores.append(mm(reader, key, ((1,), (1,))))
                inters.append(mm(reader, state[:, cols].astype(BF16), ((1,), (1,))))
                updates.append(mm(value[rows, cols], key, ((0,), (0,))))
                decays.append(grow[BLOCK - 1 :, :])
            for h, cols in enumerate(head_cols):
                gating_out[rows, cols] = (
                    jax.nn.silu(gate[rows, cols].astype(F32)) * gain[:, cols]
                )
                score = jnp.where(causal, scores[h], 0.0).astype(BF16)
                raw_out[rows, cols] = mm(score, value[rows, cols]) + inters[h]
                state[:, cols] = decays[h] * (state[:, cols] + updates[h])
                decay[:, cols] = decay[:, cols] * decays[h]
        return carry

    lax.fori_loop(0, blocks // unroll, advance, 0)

    deal = deal_matrix(plane, depth, False)
    for h in range(heads):
        cols = pl.ds(h * 128, 128)
        dealt = mm(deal, state[:, cols].astype(BF16), ((1,), (1,)))
        send_out[:, h * depth : (h + 1) * depth, :] = (
            dealt.reshape(plane, depth, 128).astype(BF16)
        )
        whole = decay[:, cols]
        high = whole.astype(BF16).astype(F32)
        pair[h : h + 1, :] = high
        pair[heads + h : heads + h + 1, :] = whole - high
    tail = pair[...].astype(BF16)
    for p in range(plane):
        send_out[p, heads * depth :, :] = tail


SMEM_SPEC = pl.BlockSpec(memory_space=pltpu.SMEM)
VMEM_SPEC = pl.BlockSpec(memory_space=pltpu.VMEM)
HBM_SPEC = pl.BlockSpec(memory_space=pltpu.HBM)


def in_hbm(*arrays):
    return [pltpu.with_memory_space_constraint(array, pltpu.HBM) for array in arrays]


def stretch(gap, gain, query, logit, value, gate, heads, plane, depth, unroll):
    span, width = query.shape
    steps = span // BLOCK // unroll
    return pl.pallas_call(
        functools.partial(stretch_kernel, heads, plane, depth, unroll),
        in_specs=[HBM_SPEC] * 6,
        out_specs=[VMEM_SPEC] * 4,
        out_shape=[
            jax.ShapeDtypeStruct((span, width), F32),
            jax.ShapeDtypeStruct((span, width), BF16),
            jax.ShapeDtypeStruct((span, width), F32),
            jax.ShapeDtypeStruct((plane, heads * depth + 2 * heads, 128), BF16),
        ],
        scratch_shapes=[pltpu.VMEM((span, width), BF16)] * 4
        + [pltpu.VMEM((span, width), F32)] * 2
        + [
            pltpu.VMEM((1, width), F32),
            pltpu.VMEM((1, width), F32),
            pltpu.VMEM((128, width), F32),
            pltpu.VMEM((1, width), F32),
            pltpu.VMEM((2 * heads, 128), F32),
            pltpu.SemaphoreType.DMA((4, steps)),
            pltpu.SemaphoreType.DMA((2,)),
        ],
        compiler_params=pltpu.CompilerParams(vmem_limit_bytes=28 * 1024 * 1024),
        cost_estimate=pl.CostEstimate(flops=6_000_000_000, bytes_accessed=10_000_000, transcendentals=0),
        name="stretch",
    )(*in_hbm(gap, gain, query, logit, value, gate))


def decay_columns(place, received, heads, depth, plane):
    count = received.shape[0]
    picked = (iota((depth, 128), 1) == iota((depth, 128), 0) * plane + place).astype(BF16)
    parts = received[:, heads * depth :, :].reshape(count * 2 * heads, 128)
    columns = mm(picked, parts, ((1,), (1,)))
    lanes = columns.shape[1]
    return columns + pltpu.roll(columns, lanes - heads, 1)


def plane_kernel(heads, plane, depth, place, received, send_out, prefix_out, product_out):
    columns = decay_columns(place[0], received, heads, depth, plane)
    total = None
    states = [jnp.zeros((depth, 128), F32) for _ in range(heads)]
    products = [jnp.ones((depth, 128), F32) for _ in range(heads)]
    for s in range(plane):
        parts = received[s, heads * depth :, :].astype(F32)
        row_decay = parts + pltpu.roll(parts, heads, 0)
        total = row_decay if total is None else total * row_decay
        for h in range(heads):
            rows = slice(h * depth, (h + 1) * depth)
            prefix_out[s, rows, :] = states[h]
            product_out[s, rows, :] = products[h]
            lane = s * 2 * heads + h
            decay = jnp.broadcast_to(columns[:, lane : lane + 1], (depth, 128))
            states[h] = decay * states[h] + received[s, rows, :].astype(F32)
            products[h] = decay * products[h]
    high = total.astype(BF16).astype(F32)
    tail = jnp.where(iota(total.shape, 0) < heads, high, total - high).astype(BF16)
    for d in range(send_out.shape[0]):
        for h in range(heads):
            send_out[d, h * depth : (h + 1) * depth, :] = states[h].astype(BF16)
        send_out[d, heads * depth :, :] = tail


def plane_scan(place, received, heads, depth):
    plane, tall, _ = received.shape
    rows = heads * depth
    return pl.pallas_call(
        functools.partial(plane_kernel, heads, plane, depth),
        in_specs=[SMEM_SPEC, VMEM_SPEC],
        out_specs=[VMEM_SPEC] * 3,
        out_shape=[
            jax.ShapeDtypeStruct((depth, tall, 128), BF16),
            jax.ShapeDtypeStruct((plane, rows, 128), F32),
            jax.ShapeDtypeStruct((plane, rows, 128), F32),
        ],
        compiler_params=pltpu.CompilerParams(vmem_limit_bytes=8 * 1024 * 1024),
        cost_estimate=pl.CostEstimate(flops=100_000_000, bytes_accessed=1_000_000, transcendentals=0),
        name="plane_scan",
    )(place, received)


def depth_kernel(heads, plane, depth, place, received, prefix, product, first,
                 send_out, final_out, entering, final):
    columns = decay_columns(place[0], received, heads, depth, plane)
    states = [first[h, pl.ds(place[0], depth, stride=plane), :] for h in range(heads)]
    for s in range(depth):
        for h in range(heads):
            rows = slice(h * depth, (h + 1) * depth)
            entering[s, rows, :] = states[h]
            lane = s * 2 * heads + h
            decay = jnp.broadcast_to(columns[:, lane : lane + 1], (depth, 128))
            states[h] = decay * states[h] + received[s, rows, :].astype(F32)
    for h in range(heads):
        final[h] = states[h]
        final_out[h : h + 1, :] = final[h, pl.ds(place[1], 1), :]
    mine = entering[place[1]]
    for p in range(plane):
        send_out[p] = (prefix[p] + product[p] * mine).astype(BF16)


def depth_scan(place, received, prefix, product, first, heads):
    depth, tall, _ = received.shape
    plane, rows, _ = prefix.shape
    return pl.pallas_call(
        functools.partial(depth_kernel, heads, plane, depth),
        in_specs=[SMEM_SPEC] + [VMEM_SPEC] * 4,
        out_specs=[VMEM_SPEC] * 2,
        out_shape=[
            jax.ShapeDtypeStruct((plane, rows, 128), BF16),
            jax.ShapeDtypeStruct((heads, 128), F32),
        ],
        scratch_shapes=[
            pltpu.VMEM((depth, rows, 128), F32),
            pltpu.VMEM((heads, depth, 128), F32),
        ],
        compiler_params=pltpu.CompilerParams(vmem_limit_bytes=8 * 1024 * 1024),
        cost_estimate=pl.CostEstimate(flops=100_000_000, bytes_accessed=1_000_000, transcendentals=0),
        name="depth_scan",
    )(place, received, prefix, product, first)


def finish_kernel(heads, depth, half, incoming, raw, reach, gating, gated_out, state):
    plane = incoming.shape[0]

    @pl.when(pl.program_id(0) == 0)
    def _():
        collect = deal_matrix(plane, depth, True)
        for h in range(heads):
            part = incoming[:, h * depth : (h + 1) * depth, :].astype(F32)
            part = part.reshape(plane * depth, 128).astype(BF16)
            state[h] = mm(collect, part).astype(BF16)

    mean = jnp.full((128, 128), 1.0 / 128, BF16)
    for b in range(raw.shape[0] // BLOCK):
        rows = pl.ds(b * BLOCK, BLOCK)
        for h in range(heads):
            cols = pl.ds(h * 128, 128)
            value = raw[rows, cols] + mm(reach[rows, cols], state[h])
            mean_square = mm((value * value).astype(BF16), mean)
            gated_out[rows, cols] = (
                value * lax.rsqrt(mean_square + EPSILON) * gating[rows, cols]
            ).astype(BF16)


def finish(half, incoming, raw, reach, gating, heads, depth, rows):
    span, width = raw.shape
    steps = span // 2 // rows
    tall = pl.BlockSpec((rows, width), lambda i, w: (w[0] * steps + i, 0))
    return pl.pallas_call(
        functools.partial(finish_kernel, heads, depth),
        grid_spec=pltpu.PrefetchScalarGridSpec(
            num_scalar_prefetch=1,
            grid=(steps,),
            in_specs=[pl.BlockSpec(incoming.shape, lambda i, w: (0, 0, 0)), tall, tall, tall],
            out_specs=pl.BlockSpec((rows, width), lambda i, w: (i, 0)),
            scratch_shapes=[pltpu.VMEM((heads, 128, 128), BF16)],
        ),
        out_shape=jax.ShapeDtypeStruct((span // 2, width), BF16),
        compiler_params=params(12),
        cost_estimate=pl.CostEstimate(flops=2_000_000_000, bytes_accessed=4_000_000, transcendentals=0),
        name="finish",
    )(half, incoming, raw, reach, gating)


def project_kernel(mine, theirs, my_weight, their_weight, out):
    total = mm(mine[...], my_weight[...]) + mm(theirs[...], their_weight[...])
    out[...] = total.astype(BF16)


def project(mine, theirs, my_weight, their_weight, rows):
    total, inner = mine.shape
    width = my_weight.shape[1]
    left = pl.BlockSpec((rows, inner), lambda i: (i, 0))
    right = pl.BlockSpec((inner, width), lambda i: (0, 0))
    return pl.pallas_call(
        project_kernel,
        grid=(total // rows,),
        in_specs=[left, left, right, right],
        out_specs=pl.BlockSpec((rows, width), lambda i: (i, 0)),
        out_shape=jax.ShapeDtypeStruct((total, width), BF16),
        compiler_params=params(20),
        cost_estimate=pl.CostEstimate(flops=3_300_000_000, bytes_accessed=9_000_000, transcendentals=0),
        name="project",
    )(mine, theirs, my_weight, their_weight)


def per_device(
    queries, forget_logit, value_rows, out_gate, floor_gap, head_gain, state_in, out_weight
):
    heads = state_in.shape[0]
    plane = lax.axis_size(PLANE)
    depth = lax.axis_size(Z)
    place_plane = lax.axis_index(PLANE)
    place = jnp.stack([place_plane, lax.axis_index(Z)]).astype(jnp.int32)
    core = lax.axis_index("tp")
    other_half = (1 - core).reshape(1).astype(jnp.int32)
    my_half = core.reshape(1).astype(jnp.int32)
    swap = [(0, 1), (1, 0)]
    barrier = lax.optimization_barrier

    gap = floor_gap.reshape(1, -1)
    gain = head_gain.reshape(1, -1)
    gap, place, my_half, other_half = barrier((gap, place, my_half, other_half))

    *local, send = stretch(
        gap, gain, queries, forget_logit, value_rows, out_gate, heads, plane, depth, UNROLL
    )
    send, out_weight = barrier((send, out_weight))
    their_weight = lax.ppermute(out_weight, "tp", swap)
    received = lax.all_to_all(send, PLANE, 0, 0, tiled=True)

    send, prefix, product = plane_scan(place, received, heads, depth)
    received = lax.all_to_all(send, Z, 0, 0, tiled=True)
    send, state_out = depth_scan(place, received, prefix, product, state_in, heads)
    incoming = lax.all_to_all(send, PLANE, 0, 0, tiled=True)

    far_gated = finish(other_half, incoming, *local, heads, depth, 384)
    theirs = lax.ppermute(far_gated, "tp", swap)
    mine = finish(my_half, incoming, *local, heads, depth, 384)
    projected = project(mine, theirs, out_weight, their_weight, 256)
    return (projected, state_out)


def solution(mesh):
    torus = Mesh(mesh.devices.reshape(8, 4, 4, mesh.shape["tp"]), (Z, Y, X, "tp"))
    placed = (
        P(SP, "tp"),
        P(SP, "tp"),
        P(SP, "tp"),
        P(SP, "tp"),
        P("tp"),
        P("tp"),
        P("tp", None, None),
        P("tp", None),
    )
    return jax.shard_map(
        per_device,
        mesh=torus,
        in_specs=placed,
        out_specs=(P(SP_TP, None), P("tp", SP)),
        check_vma=False,
    )
```

```python
import functools

import jax
import jax.numpy as jnp
from jax import lax
from jax.experimental import pallas as pl
from jax.experimental.pallas import tpu as pltpu
from jax.sharding import Mesh
from jax.sharding import PartitionSpec as P

BLOCK = 128
UNROLL = 4
EPSILON = 1e-06
LOG2E = 1.4426950408889634
Z, Y, X = ("sp_0", "sp_1", "sp_2")
SP = (Z, Y, X)
PLANE = (Y, X)
SP_TP = (Z, Y, X, "tp")
F32 = jnp.float32
BF16 = jnp.bfloat16


def mm(a, b, dims=((1,), (0,))):
    return lax.dot_general(a, b, (dims, ((), ())), preferred_element_type=F32)


def iota(shape, axis):
    return lax.broadcasted_iota(jnp.int32, shape, axis)


def params(limit_mib):
    return pltpu.CompilerParams(
        dimension_semantics=("arbitrary",), vmem_limit_bytes=limit_mib * 1024 * 1024
    )


def deal_matrix(plane, depth, transposed):
    rows = plane * depth
    dealt = iota((rows, rows), 1 if transposed else 0)
    natural = iota((rows, rows), 0 if transposed else 1)
    return ((dealt % depth) * plane + dealt // depth == natural).astype(BF16)


def log2_of_rest(gate):
    near = gate * (gate * (gate * (-LOG2E / 3) - LOG2E / 2) - LOG2E)
    return jnp.where(gate < 1e-3, near, jnp.log2(1.0 - gate))


def stretch_kernel(heads, plane, depth, unroll, gap_in, gain_in, query_in, logit_in, value_in,
                   gate_in, raw_out, reach_out, gating_out, send_out,
                   query, logit, value, gate, key_gates, cumuls, gap, gain, state, decay, pair, sems, small_sems):
    blocks = query.shape[0] // BLOCK
    sides = ((value_in, value), (query_in, query), (gate_in, gate))
    rest = [
        pltpu.make_async_copy(source, target, small_sems.at[2 + n])
        for n, (source, target) in enumerate(sides)
    ]

    def logits(i):
        rows = pl.ds(i * unroll * BLOCK, unroll * BLOCK)
        return pltpu.make_async_copy(logit_in.at[rows, :], logit.at[rows, :], sems.at[i])

    small = [
        pltpu.make_async_copy(gap_in, gap, small_sems.at[0]),
        pltpu.make_async_copy(gain_in, gain, small_sems.at[1]),
    ]
    for copy in small:
        copy.start()
    for i in range(blocks // unroll):
        logits(i).start()
    for copy in rest:
        copy.start()
    state[...] = jnp.zeros_like(state)
    decay[...] = jnp.ones_like(decay)
    causal = iota((BLOCK, BLOCK), 0) >= iota((BLOCK, BLOCK), 1)
    lower = causal.astype(BF16)
    lower2 = jnp.concatenate([lower, lower], axis=1)
    head_cols = [pl.ds(h * 128, 128) for h in range(heads)]
    for copy in small:
        copy.wait()

    def rows_of(block):
        return pl.ds(pl.multiple_of(block * BLOCK, BLOCK), BLOCK)

    def sum_logs(i, carry):
        logits(i).wait()
        for b in range(unroll):
            rows = rows_of(i * unroll + b)
            highs, lows = [], []
            for cols in head_cols:
                key_gate = gap[:, cols] * jax.nn.sigmoid(-logit[rows, cols].astype(F32))
                key_gates[rows, cols] = key_gate
                log_forget = log2_of_rest(key_gate)
                highs.append(log_forget.astype(BF16))
                lows.append((log_forget - highs[-1].astype(F32)).astype(BF16))
            split = jnp.concatenate(
                [jnp.concatenate(highs, axis=1), jnp.concatenate(lows, axis=1)], axis=0
            )
            cumuls[rows, :] = mm(lower2, split)
        return carry

    lax.fori_loop(0, blocks // unroll, sum_logs, 0)

    for copy in rest:
        copy.wait()

    def advance(i, carry):
        for b in range(unroll):
            rows = rows_of(i * unroll + b)
            scores, inters, updates, decays = [], [], [], []
            for cols in head_cols:
                cumul = cumuls[rows, cols]
                grow = jnp.exp2(cumul)
                key = (key_gates[rows, cols] * jnp.exp2(-cumul)).astype(BF16)
                reader = jax.nn.silu(query[rows, cols].astype(F32)) * grow
                reach_out[rows, cols] = (reader * decay[:, cols]).astype(BF16)
                reader = reader.astype(BF16)
                both = jnp.concatenate([key, state[:, cols].astype(BF16)], axis=0)
                both = mm(reader, both, ((1,), (1,)))
                scores.append(both[:, :BLOCK])
                inters.append(both[:, BLOCK:])
                updates.append(mm(value[rows, cols], key, ((0,), (0,))))
                decays.append(grow[BLOCK - 1 :, :])
            for h, cols in enumerate(head_cols):
                gating_out[rows, cols] = (
                    jax.nn.silu(gate[rows, cols].astype(F32)) * gain[:, cols]
                )
                score = jnp.where(causal, scores[h], 0.0).astype(BF16)
                raw_out[rows, cols] = mm(score, value[rows, cols]) + inters[h]
                state[:, cols] = decays[h] * (state[:, cols] + updates[h])
                decay[:, cols] = decay[:, cols] * decays[h]
        return carry

    lax.fori_loop(0, blocks // unroll, advance, 0)

    deal = deal_matrix(plane, depth, False)
    for h in range(heads):
        cols = pl.ds(h * 128, 128)
        dealt = mm(deal, state[:, cols].astype(BF16), ((1,), (1,)))
        send_out[:, h * depth : (h + 1) * depth, :] = (
            dealt.reshape(plane, depth, 128).astype(BF16)
        )
        whole = decay[:, cols]
        high = whole.astype(BF16).astype(F32)
        pair[h : h + 1, :] = high
        pair[heads + h : heads + h + 1, :] = whole - high
    tail = pair[...].astype(BF16)
    for p in range(plane):
        send_out[p, heads * depth :, :] = tail


SMEM_SPEC = pl.BlockSpec(memory_space=pltpu.SMEM)
VMEM_SPEC = pl.BlockSpec(memory_space=pltpu.VMEM)
HBM_SPEC = pl.BlockSpec(memory_space=pltpu.HBM)


def in_hbm(*arrays):
    return [pltpu.with_memory_space_constraint(array, pltpu.HBM) for array in arrays]


def stretch(gap, gain, query, logit, value, gate, heads, plane, depth, unroll):
    span, width = query.shape
    steps = span // BLOCK // unroll
    return pl.pallas_call(
        functools.partial(stretch_kernel, heads, plane, depth, unroll),
        in_specs=[HBM_SPEC] * 6,
        out_specs=[VMEM_SPEC] * 4,
        out_shape=[
            jax.ShapeDtypeStruct((span, width), F32),
            jax.ShapeDtypeStruct((span, width), BF16),
            jax.ShapeDtypeStruct((span, width), F32),
            jax.ShapeDtypeStruct((plane, heads * depth + 2 * heads, 128), BF16),
        ],
        scratch_shapes=[pltpu.VMEM((span, width), BF16)] * 4
        + [pltpu.VMEM((span, width), F32)] * 2
        + [
            pltpu.VMEM((1, width), F32),
            pltpu.VMEM((1, width), F32),
            pltpu.VMEM((128, width), F32),
            pltpu.VMEM((1, width), F32),
            pltpu.VMEM((2 * heads, 128), F32),
            pltpu.SemaphoreType.DMA((steps,)),
            pltpu.SemaphoreType.DMA((5,)),
        ],
        compiler_params=pltpu.CompilerParams(vmem_limit_bytes=28 * 1024 * 1024),
        cost_estimate=pl.CostEstimate(flops=6_000_000_000, bytes_accessed=10_000_000, transcendentals=0),
        name="stretch",
    )(*in_hbm(gap, gain, query, logit, value, gate))


def decay_columns(place, received, heads, depth, plane):
    count = received.shape[0]
    picked = (iota((depth, 128), 1) == iota((depth, 128), 0) * plane + place).astype(BF16)
    parts = received[:, heads * depth :, :].reshape(count * 2 * heads, 128)
    columns = mm(picked, parts, ((1,), (1,)))
    lanes = columns.shape[1]
    return columns + pltpu.roll(columns, lanes - heads, 1)


def plane_kernel(heads, plane, depth, place, received, send_out, prefix_out, product_out):
    columns = decay_columns(place[0], received, heads, depth, plane)
    total = None
    states = [jnp.zeros((depth, 128), F32) for _ in range(heads)]
    products = [jnp.ones((depth, 128), F32) for _ in range(heads)]
    for s in range(plane):
        parts = received[s, heads * depth :, :].astype(F32)
        row_decay = parts + pltpu.roll(parts, heads, 0)
        total = row_decay if total is None else total * row_decay
        for h in range(heads):
            rows = slice(h * depth, (h + 1) * depth)
            prefix_out[s, rows, :] = states[h]
            product_out[s, rows, :] = products[h]
            lane = s * 2 * heads + h
            decay = jnp.broadcast_to(columns[:, lane : lane + 1], (depth, 128))
            states[h] = decay * states[h] + received[s, rows, :].astype(F32)
            products[h] = decay * products[h]
    high = total.astype(BF16).astype(F32)
    tail = jnp.where(iota(total.shape, 0) < heads, high, total - high).astype(BF16)
    for d in range(send_out.shape[0]):
        for h in range(heads):
            send_out[d, h * depth : (h + 1) * depth, :] = states[h].astype(BF16)
        send_out[d, heads * depth :, :] = tail


def plane_scan(place, received, heads, depth):
    plane, tall, _ = received.shape
    rows = heads * depth
    return pl.pallas_call(
        functools.partial(plane_kernel, heads, plane, depth),
        in_specs=[SMEM_SPEC, VMEM_SPEC],
        out_specs=[VMEM_SPEC] * 3,
        out_shape=[
            jax.ShapeDtypeStruct((depth, tall, 128), BF16),
            jax.ShapeDtypeStruct((plane, rows, 128), F32),
            jax.ShapeDtypeStruct((plane, rows, 128), F32),
        ],
        compiler_params=pltpu.CompilerParams(vmem_limit_bytes=8 * 1024 * 1024),
        cost_estimate=pl.CostEstimate(flops=100_000_000, bytes_accessed=1_000_000, transcendentals=0),
        name="plane_scan",
    )(place, received)


def depth_kernel(heads, plane, depth, place, received, prefix, product, first,
                 send_out, final_out, entering, final):
    columns = decay_columns(place[0], received, heads, depth, plane)
    states = [first[h, pl.ds(place[0], depth, stride=plane), :] for h in range(heads)]
    for s in range(depth):
        for h in range(heads):
            rows = slice(h * depth, (h + 1) * depth)
            entering[s, rows, :] = states[h]
            lane = s * 2 * heads + h
            decay = jnp.broadcast_to(columns[:, lane : lane + 1], (depth, 128))
            states[h] = decay * states[h] + received[s, rows, :].astype(F32)
    for h in range(heads):
        final[h] = states[h]
        final_out[h : h + 1, :] = final[h, pl.ds(place[1], 1), :]
    mine = entering[place[1]]
    for p in range(plane):
        send_out[p] = (prefix[p] + product[p] * mine).astype(BF16)


def depth_scan(place, received, prefix, product, first, heads):
    depth, tall, _ = received.shape
    plane, rows, _ = prefix.shape
    return pl.pallas_call(
        functools.partial(depth_kernel, heads, plane, depth),
        in_specs=[SMEM_SPEC] + [VMEM_SPEC] * 4,
        out_specs=[VMEM_SPEC] * 2,
        out_shape=[
            jax.ShapeDtypeStruct((plane, rows, 128), BF16),
            jax.ShapeDtypeStruct((heads, 128), F32),
        ],
        scratch_shapes=[
            pltpu.VMEM((depth, rows, 128), F32),
            pltpu.VMEM((heads, depth, 128), F32),
        ],
        compiler_params=pltpu.CompilerParams(vmem_limit_bytes=8 * 1024 * 1024),
        cost_estimate=pl.CostEstimate(flops=100_000_000, bytes_accessed=1_000_000, transcendentals=0),
        name="depth_scan",
    )(place, received, prefix, product, first)


def gather_state(heads, depth, incoming, state):
    plane = incoming.shape[0]
    collect = deal_matrix(plane, depth, True)
    for h in range(heads):
        part = incoming[:, h * depth : (h + 1) * depth, :].astype(F32)
        part = part.reshape(plane * depth, 128).astype(BF16)
        state[h] = mm(collect, part).astype(BF16)


def gated_rows(heads, rows, raw, reach, gating, state, gated_out):
    for h in range(heads):
        cols = pl.ds(h * 128, 128)
        value = raw[rows, cols] + mm(reach[rows, cols], state[h])
        mean_square = jnp.mean(value * value, axis=-1, keepdims=True)
        gated_out[rows, cols] = (
            value * lax.rsqrt(mean_square + EPSILON) * gating[rows, cols]
        ).astype(BF16)


def far_kernel(heads, depth, half, incoming, raw, reach, gating, gated_out, state):
    @pl.when(pl.program_id(0) == 0)
    def _():
        gather_state(heads, depth, incoming, state)

    for b in range(raw.shape[0] // BLOCK):
        gated_rows(heads, pl.ds(b * BLOCK, BLOCK), raw, reach, gating, state, gated_out)


def near_kernel(heads, half, state, raw, reach, gating, weight, partial_out, gated):
    for b in range(raw.shape[0] // BLOCK):
        gated_rows(heads, pl.ds(b * BLOCK, BLOCK), raw, reach, gating, state, gated)
    partial_out[...] = mm(gated[...], weight[...])


def far_rows(half, incoming, raw, reach, gating, heads, depth, rows):
    span, width = raw.shape
    steps = span // 2 // rows
    tall = pl.BlockSpec((rows, width), lambda i, w: (w[0] * steps + i, 0))
    return pl.pallas_call(
        functools.partial(far_kernel, heads, depth),
        grid_spec=pltpu.PrefetchScalarGridSpec(
            num_scalar_prefetch=1,
            grid=(steps,),
            in_specs=[pl.BlockSpec(incoming.shape, lambda i, w: (0, 0, 0)), tall, tall, tall],
            out_specs=[
                pl.BlockSpec((rows, width), lambda i, w: (i, 0)),
                pl.BlockSpec((heads, 128, 128), lambda i, w: (0, 0, 0)),
            ],
        ),
        out_shape=[
            jax.ShapeDtypeStruct((span // 2, width), BF16),
            jax.ShapeDtypeStruct((heads, 128, 128), BF16),
        ],
        compiler_params=params(12),
        cost_estimate=pl.CostEstimate(flops=2_000_000_000, bytes_accessed=4_000_000, transcendentals=0),
        name="far_rows",
    )(half, incoming, raw, reach, gating)


def near_rows(half, state, raw, reach, gating, weight, heads, rows):
    span, width = raw.shape
    inner, out_width = weight.shape
    steps = span // 2 // rows
    tall = pl.BlockSpec((rows, width), lambda i, w: (w[0] * steps + i, 0))
    return pl.pallas_call(
        functools.partial(near_kernel, heads),
        grid_spec=pltpu.PrefetchScalarGridSpec(
            num_scalar_prefetch=1,
            grid=(steps,),
            in_specs=[
                pl.BlockSpec(state.shape, lambda i, w: (0, 0, 0)),
                tall,
                tall,
                tall,
                pl.BlockSpec((inner, out_width), lambda i, w: (0, 0)),
            ],
            out_specs=pl.BlockSpec((rows, out_width), lambda i, w: (i, 0)),
            scratch_shapes=[pltpu.VMEM((rows, width), BF16)],
        ),
        out_shape=jax.ShapeDtypeStruct((span // 2, out_width), F32),
        compiler_params=params(20),
        cost_estimate=pl.CostEstimate(flops=4_000_000_000, bytes_accessed=4_000_000, transcendentals=0),
        name="near_rows",
    )(half, state, raw, reach, gating, weight)


def project_kernel(partial, theirs, their_weight, final, out, final_out):
    out[...] = (partial[...] + mm(theirs[...], their_weight[...])).astype(BF16)
    final_out[...] = final[...]


def project(partial, theirs, their_weight, final, rows):
    total, width = partial.shape
    inner = theirs.shape[1]
    whole = pl.BlockSpec(final.shape, lambda i: (0, 0))
    return pl.pallas_call(
        project_kernel,
        grid=(total // rows,),
        in_specs=[
            pl.BlockSpec((rows, width), lambda i: (i, 0)),
            pl.BlockSpec((rows, inner), lambda i: (i, 0)),
            pl.BlockSpec((inner, width), lambda i: (0, 0)),
            whole,
        ],
        out_specs=[pl.BlockSpec((rows, width), lambda i: (i, 0)), whole],
        out_shape=[
            jax.ShapeDtypeStruct((total, width), BF16),
            jax.ShapeDtypeStruct(final.shape, F32),
        ],
        compiler_params=params(20),
        cost_estimate=pl.CostEstimate(flops=3_300_000_000, bytes_accessed=9_000_000, transcendentals=0),
        name="project",
    )(partial, theirs, pltpu.with_memory_space_constraint(their_weight, pltpu.VMEM), final)


def per_device(
    queries, forget_logit, value_rows, out_gate, floor_gap, head_gain, state_in, out_weight
):
    heads = state_in.shape[0]
    plane = lax.axis_size(PLANE)
    depth = lax.axis_size(Z)
    place_plane = lax.axis_index(PLANE)
    place = jnp.stack([place_plane, lax.axis_index(Z)]).astype(jnp.int32)
    core = lax.axis_index("tp")
    other_half = (1 - core).reshape(1).astype(jnp.int32)
    my_half = core.reshape(1).astype(jnp.int32)
    swap = [(0, 1), (1, 0)]
    barrier = lax.optimization_barrier

    gap = floor_gap.reshape(1, -1)
    gain = head_gain.reshape(1, -1)
    gap, place, my_half, other_half = barrier((gap, place, my_half, other_half))

    *local, send = stretch(
        gap, gain, queries, forget_logit, value_rows, out_gate, heads, plane, depth, UNROLL
    )
    send, out_weight = barrier((send, out_weight))
    their_weight = lax.ppermute(out_weight, "tp", swap)
    received = lax.all_to_all(send, PLANE, 0, 0, tiled=True)

    send, prefix, product = plane_scan(place, received, heads, depth)
    received = lax.all_to_all(send, Z, 0, 0, tiled=True)
    send, final = depth_scan(place, received, prefix, product, state_in, heads)
    incoming = lax.all_to_all(send, PLANE, 0, 0, tiled=True)

    far, state = far_rows(other_half, incoming, *local, heads, depth, 384)
    theirs = lax.ppermute(far, "tp", swap)
    partial = near_rows(my_half, state, *local, out_weight, heads, 384)
    projected, state_out = project(partial, theirs, their_weight, final, 256)
    return (projected, state_out)


def solution(mesh):
    torus = Mesh(mesh.devices.reshape(8, 4, 4, mesh.shape["tp"]), (Z, Y, X, "tp"))
    placed = (
        P(SP, "tp"),
        P(SP, "tp"),
        P(SP, "tp"),
        P(SP, "tp"),
        P("tp"),
        P("tp"),
        P("tp", None, None),
        P("tp", None),
    )
    return jax.shard_map(
        per_device,
        mesh=torus,
        in_specs=placed,
        out_specs=(P(SP_TP, None), P("tp", SP)),
        check_vma=False,
    )
```

```python
import functools

import jax
import jax.numpy as jnp
from jax import lax
from jax.experimental import pallas as pl
from jax.experimental.pallas import tpu as pltpu
from jax.sharding import Mesh
from jax.sharding import PartitionSpec as P

BLOCK = 128
UNROLL = 4
EPSILON = 1e-06
LOG2E = 1.4426950408889634
Z, Y, X = ("sp_0", "sp_1", "sp_2")
SP = (Z, Y, X)
PLANE = (Y, X)
SP_TP = (Z, Y, X, "tp")
F32 = jnp.float32
BF16 = jnp.bfloat16


def mm(a, b, dims=((1,), (0,))):
    return lax.dot_general(a, b, (dims, ((), ())), preferred_element_type=F32)


def iota(shape, axis):
    return lax.broadcasted_iota(jnp.int32, shape, axis)


def params(limit_mib):
    return pltpu.CompilerParams(
        dimension_semantics=("arbitrary",), vmem_limit_bytes=limit_mib * 1024 * 1024
    )


def deal_matrix(plane, depth, transposed):
    rows = plane * depth
    dealt = iota((rows, rows), 1 if transposed else 0)
    natural = iota((rows, rows), 0 if transposed else 1)
    return ((dealt % depth) * plane + dealt // depth == natural).astype(BF16)


def log2_of_rest(gate):
    near = gate * (gate * (-LOG2E / 2) - LOG2E)
    return jnp.where(gate < 1e-3, near, jnp.log2(1.0 - gate))


def goes_early(depth):
    return lax.axis_index(Z) < depth * 3 // 8


def rows_of(block):
    return pl.ds(pl.multiple_of(block * BLOCK, BLOCK), BLOCK)


def read_block(rows, cols, query, gate, gain, cumul, offset, key, state):
    reader = jax.nn.silu(query[rows, cols].astype(F32)) * jnp.exp2(cumul)
    reach = (reader * offset).astype(BF16)
    both = mm(reader.astype(BF16), jnp.concatenate([key, state], axis=0), ((1,), (1,)))
    gating = jax.nn.silu(gate[rows, cols].astype(F32)) * gain[:, cols]
    return both, reach, gating


def finish_block(causal, both, values):
    scores = jnp.where(causal, both[:, :BLOCK], 0.0).astype(BF16)
    return mm(scores, values) + both[:, BLOCK:]


def stretch_kernel(heads, plane, depth, unroll, gap_in, gain_in, query_in, logit_in, value_in,
                   gate_in, raw_out, reach_out, gating_out, send_out, query, value, gate, cumuls,
                   keys, starts, offsets, gain, logit, key_gates, gap, state, decay, pair,
                   sems, small_sems):
    blocks = query.shape[0] // BLOCK
    sides = ((value_in, value), (query_in, query), (gate_in, gate))
    rest = [
        pltpu.make_async_copy(source, target, small_sems.at[2 + n])
        for n, (source, target) in enumerate(sides)
    ]

    def logits(i):
        rows = pl.ds(i * unroll * BLOCK, unroll * BLOCK)
        return pltpu.make_async_copy(logit_in.at[rows, :], logit.at[rows, :], sems.at[i])

    small = [
        pltpu.make_async_copy(gap_in, gap, small_sems.at[0]),
        pltpu.make_async_copy(gain_in, gain, small_sems.at[1]),
    ]
    for copy in small:
        copy.start()
    for i in range(blocks // unroll):
        logits(i).start()
    for copy in rest:
        copy.start()
    state[...] = jnp.zeros_like(state)
    decay[...] = jnp.ones_like(decay)
    causal = iota((BLOCK, BLOCK), 0) >= iota((BLOCK, BLOCK), 1)
    lower = causal.astype(BF16)
    lower2 = jnp.concatenate([lower, lower], axis=1)
    head_cols = [pl.ds(h * 128, 128) for h in range(heads)]
    for copy in small:
        copy.wait()

    half_gap = 0.5 * gap[...]

    def sum_logs(i, carry):
        logits(i).wait()
        for b in range(unroll):
            rows = rows_of(i * unroll + b)
            highs, lows = [], []
            for h, cols in enumerate(head_cols):
                key_gate = half_gap[:, h * 128 : (h + 1) * 128] * (1.0 - jnp.tanh(0.5 * logit[rows, cols].astype(F32)))
                key_gates[rows, cols] = key_gate
                log_forget = log2_of_rest(key_gate)
                highs.append(log_forget.astype(BF16))
                lows.append((log_forget - highs[-1].astype(F32)).astype(BF16))
            split = jnp.concatenate(
                [jnp.concatenate(highs, axis=1), jnp.concatenate(lows, axis=1)], axis=0
            )
            cumuls[rows, :] = mm(lower2, split)
        return carry

    lax.fori_loop(0, blocks // unroll, sum_logs, 0)
    rest[0].wait()

    def advance(whole, i, carry):
        for b in range(unroll):
            block = i * unroll + b
            rows = rows_of(block)
            boths, updates, decays = [], [], []
            for cols in head_cols:
                cumul = cumuls[rows, cols]
                key = (key_gates[rows, cols] * jnp.exp2(-cumul)).astype(BF16)
                start = state[:, cols].astype(BF16)
                if whole:
                    both, reach_out[rows, cols], gating_out[rows, cols] = read_block(
                        rows, cols, query, gate, gain, cumul, decay[:, cols], key, start
                    )
                    boths.append(both)
                else:
                    keys[rows, cols] = key
                    starts[block, :, cols] = start
                    offsets[block, :, cols] = decay[:, cols]
                updates.append(mm(value[rows, cols], key, ((0,), (0,))))
                decays.append(jnp.exp2(cumul[BLOCK - 1 :, :]))
            for h, cols in enumerate(head_cols):
                if whole:
                    raw_out[rows, cols] = finish_block(causal, boths[h], value[rows, cols])
                state[:, cols] = decays[h] * (state[:, cols] + updates[h])
                decay[:, cols] = decay[:, cols] * decays[h]
        return carry

    early = goes_early(depth)

    @pl.when(early)
    def _():
        for copy in rest[1:]:
            copy.wait()
        lax.fori_loop(0, blocks // unroll, functools.partial(advance, True), 0)

    @pl.when(jnp.logical_not(early))
    def _():
        lax.fori_loop(0, blocks // unroll, functools.partial(advance, False), 0)
        for copy in rest[1:]:
            copy.wait()

    deal = deal_matrix(plane, depth, False)
    for h in range(heads):
        cols = pl.ds(h * 128, 128)
        dealt = mm(deal, state[:, cols].astype(BF16), ((1,), (1,)))
        send_out[:, h * depth : (h + 1) * depth, :] = (
            dealt.reshape(plane, depth, 128).astype(BF16)
        )
        whole = decay[:, cols]
        high = whole.astype(BF16).astype(F32)
        pair[h : h + 1, :] = high
        pair[heads + h : heads + h + 1, :] = whole - high
    tail = pair[...].astype(BF16)
    for p in range(plane):
        send_out[p, heads * depth :, :] = tail


def late_outputs(heads, query, value, gate, cumuls, keys, starts, offsets, gain,
                 raw_out, reach_out, gating_out):
    blocks = query.shape[0] // BLOCK
    causal = iota((BLOCK, BLOCK), 0) >= iota((BLOCK, BLOCK), 1)
    head_cols = [pl.ds(h * 128, 128) for h in range(heads)]

    def step(i, carry):
        for b in range(UNROLL):
            block = i * UNROLL + b
            rows = rows_of(block)
            boths = []
            for cols in head_cols:
                both, reach_out[rows, cols], gating_out[rows, cols] = read_block(
                    rows, cols, query, gate, gain, cumuls[rows, cols], offsets[block, :, cols],
                    keys[rows, cols], starts[block, :, cols],
                )
                boths.append(both)
            for both, cols in zip(boths, head_cols):
                raw_out[rows, cols] = finish_block(causal, both, value[rows, cols])
        return carry

    lax.fori_loop(0, blocks // UNROLL, step, 0)


VMEM_SPEC = pl.BlockSpec(memory_space=pltpu.VMEM)
HBM_SPEC = pl.BlockSpec(memory_space=pltpu.HBM)


def in_hbm(*arrays):
    return [pltpu.with_memory_space_constraint(array, pltpu.HBM) for array in arrays]


def stretch(gap, gain, query, logit, value, gate, heads, plane, depth, unroll):
    span, width = query.shape
    steps = span // BLOCK // unroll
    narrow = jax.ShapeDtypeStruct((span, width), BF16)
    wide = jax.ShapeDtypeStruct((span, width), F32)
    results = pl.pallas_call(
        functools.partial(stretch_kernel, heads, plane, depth, unroll),
        in_specs=[HBM_SPEC] * 6,
        out_specs=[VMEM_SPEC] * 12,
        out_shape=[
            wide,
            narrow,
            wide,
            jax.ShapeDtypeStruct((plane, heads * depth + 2 * heads, 128), BF16),
            narrow,
            narrow,
            narrow,
            wide,
            narrow,
            jax.ShapeDtypeStruct((span // BLOCK, 128, width), BF16),
            jax.ShapeDtypeStruct((span // BLOCK, 1, width), F32),
            jax.ShapeDtypeStruct((1, width), F32),
        ],
        scratch_shapes=[
            pltpu.VMEM((span, width), BF16),
            pltpu.VMEM((span, width), F32),
            pltpu.VMEM((1, width), F32),
            pltpu.VMEM((128, width), F32),
            pltpu.VMEM((1, width), F32),
            pltpu.VMEM((2 * heads, 128), F32),
            pltpu.SemaphoreType.DMA((steps,)),
            pltpu.SemaphoreType.DMA((5,)),
        ],
        compiler_params=pltpu.CompilerParams(vmem_limit_bytes=34 * 1024 * 1024),
        cost_estimate=pl.CostEstimate(flops=6_000_000_000, bytes_accessed=10_000_000, transcendentals=0),
        name="stretch",
    )(*in_hbm(gap, gain, query, logit, value, gate))
    return results[:3], results[3], results[4:]


def decay_columns(place, received, heads, depth, plane):
    count = received.shape[0]
    picked = (iota((depth, 128), 1) == iota((depth, 128), 0) * plane + place).astype(BF16)
    parts = received[:, heads * depth :, :].reshape(count * 2 * heads, 128)
    columns = mm(picked, parts, ((1,), (1,)))
    lanes = columns.shape[1]
    return columns + pltpu.roll(columns, lanes - heads, 1)


def plane_kernel(heads, plane, depth, received, send_out, prefix_out, product_out):
    columns = decay_columns(lax.axis_index(PLANE), received, heads, depth, plane)
    total = None
    states = [jnp.zeros((depth, 128), F32) for _ in range(heads)]
    products = [jnp.ones((depth, 128), F32) for _ in range(heads)]
    for s in range(plane):
        parts = received[s, heads * depth :, :].astype(F32)
        row_decay = parts + pltpu.roll(parts, heads, 0)
        total = row_decay if total is None else total * row_decay
        for h in range(heads):
            rows = slice(h * depth, (h + 1) * depth)
            prefix_out[s, rows, :] = states[h]
            product_out[s, rows, :] = products[h]
            lane = s * 2 * heads + h
            decay = jnp.broadcast_to(columns[:, lane : lane + 1], (depth, 128))
            states[h] = decay * states[h] + received[s, rows, :].astype(F32)
            products[h] = decay * products[h]
    high = total.astype(BF16).astype(F32)
    tail = jnp.where(iota(total.shape, 0) < heads, high, total - high).astype(BF16)
    for d in range(send_out.shape[0]):
        for h in range(heads):
            send_out[d, h * depth : (h + 1) * depth, :] = states[h].astype(BF16)
        send_out[d, heads * depth :, :] = tail


def plane_scan(received, heads, depth):
    plane, tall, _ = received.shape
    rows = heads * depth
    return pl.pallas_call(
        functools.partial(plane_kernel, heads, plane, depth),
        in_specs=[VMEM_SPEC],
        out_specs=[VMEM_SPEC] * 3,
        out_shape=[
            jax.ShapeDtypeStruct((depth, tall, 128), BF16),
            jax.ShapeDtypeStruct((plane, rows, 128), F32),
            jax.ShapeDtypeStruct((plane, rows, 128), F32),
        ],
        compiler_params=pltpu.CompilerParams(vmem_limit_bytes=8 * 1024 * 1024),
        cost_estimate=pl.CostEstimate(flops=100_000_000, bytes_accessed=1_000_000, transcendentals=0),
        name="plane_scan",
    )(received)


def depth_kernel(heads, plane, depth, received, prefix, product, first, query, value, gate,
                 cumuls, keys, starts, offsets, gain, raw_in, reach_in, gating_in,
                 send_out, final_out, raw_out, reach_out, gating_out, entering, final):
    columns = decay_columns(lax.axis_index(PLANE), received, heads, depth, plane)
    states = [first[h, pl.ds(lax.axis_index(PLANE), depth, stride=plane), :] for h in range(heads)]
    for s in range(depth):
        for h in range(heads):
            rows = slice(h * depth, (h + 1) * depth)
            entering[s, rows, :] = states[h]
            lane = s * 2 * heads + h
            decay = jnp.broadcast_to(columns[:, lane : lane + 1], (depth, 128))
            states[h] = decay * states[h] + received[s, rows, :].astype(F32)
    for h in range(heads):
        final[h] = states[h]
        final_out[h : h + 1, :] = final[h, pl.ds(lax.axis_index(Z), 1), :]
    mine = entering[lax.axis_index(Z)]
    for p in range(plane):
        send_out[p] = (prefix[p] + product[p] * mine).astype(BF16)

    @pl.when(jnp.logical_not(goes_early(depth)))
    def _():
        late_outputs(heads, query, value, gate, cumuls, keys, starts, offsets, gain,
                     raw_out, reach_out, gating_out)


def depth_scan(received, prefix, product, first, left, local, heads):
    depth, tall, _ = received.shape
    plane, rows, _ = prefix.shape
    return pl.pallas_call(
        functools.partial(depth_kernel, heads, plane, depth),
        in_specs=[VMEM_SPEC] * 15,
        out_specs=[VMEM_SPEC] * 5,
        out_shape=[
            jax.ShapeDtypeStruct((plane, rows, 128), BF16),
            jax.ShapeDtypeStruct((heads, 128), F32),
        ]
        + [jax.ShapeDtypeStruct(array.shape, array.dtype) for array in local],
        input_output_aliases={12: 2, 13: 3, 14: 4},
        scratch_shapes=[
            pltpu.VMEM((depth, rows, 128), F32),
            pltpu.VMEM((heads, depth, 128), F32),
        ],
        compiler_params=pltpu.CompilerParams(vmem_limit_bytes=30 * 1024 * 1024),
        cost_estimate=pl.CostEstimate(flops=100_000_000, bytes_accessed=1_000_000, transcendentals=0),
        name="depth_scan",
    )(received, prefix, product, first, *left, *local)


def gather_state(heads, depth, incoming, state):
    plane = incoming.shape[0]
    collect = deal_matrix(plane, depth, True)
    for h in range(heads):
        part = incoming[:, h * depth : (h + 1) * depth, :].astype(F32)
        part = part.reshape(plane * depth, 128).astype(BF16)
        state[h] = mm(collect, part).astype(BF16)


def gated_block(heads, source, raw, reach, gating, state, gated_out, target):
    rows = pl.ds(pl.multiple_of(source, BLOCK), BLOCK)
    for h in range(heads):
        cols = pl.ds(h * 128, 128)
        value = raw[rows, cols] + mm(reach[rows, cols], state[h])
        mean_square = jnp.mean(value * value, axis=-1, keepdims=True)
        gated_out[target : target + BLOCK, cols] = (
            value * lax.rsqrt(mean_square + EPSILON) * gating[rows, cols]
        ).astype(BF16)


def far_kernel(heads, depth, incoming, raw, reach, gating, gated_out, state):
    gather_state(heads, depth, incoming, state)
    half = gated_out.shape[0]
    first = (1 - lax.axis_index("tp")) * half
    for row in range(0, half, BLOCK):
        gated_block(heads, first + row, raw, reach, gating, state, gated_out, row)


def near_kernel(heads, tall, state, raw, reach, gating, weight, partial_out, gated):
    half = partial_out.shape[0]
    first = lax.axis_index("tp") * half
    for row in range(0, half, BLOCK):
        gated_block(heads, first + row, raw, reach, gating, state, gated, row)
        if (row + BLOCK) % tall == 0:
            done = pl.ds(row + BLOCK - tall, tall)
            partial_out[done, :] = mm(gated[done, :], weight[...])


def far_rows(incoming, raw, reach, gating, heads, depth):
    span, width = raw.shape
    return pl.pallas_call(
        functools.partial(far_kernel, heads, depth),
        in_specs=[VMEM_SPEC] * 4,
        out_specs=[VMEM_SPEC] * 2,
        out_shape=[
            jax.ShapeDtypeStruct((span // 2, width), BF16),
            jax.ShapeDtypeStruct((heads, 128, 128), BF16),
        ],
        compiler_params=pltpu.CompilerParams(vmem_limit_bytes=12 * 1024 * 1024),
        cost_estimate=pl.CostEstimate(flops=2_000_000_000, bytes_accessed=4_000_000, transcendentals=0),
        name="far_rows",
    )(incoming, raw, reach, gating)


def near_rows(state, raw, reach, gating, weight, heads, rows):
    span, width = raw.shape
    return pl.pallas_call(
        functools.partial(near_kernel, heads, rows),
        in_specs=[VMEM_SPEC] * 5,
        out_specs=VMEM_SPEC,
        out_shape=jax.ShapeDtypeStruct((span // 2, weight.shape[1]), F32),
        scratch_shapes=[pltpu.VMEM((span // 2, width), BF16)],
        compiler_params=pltpu.CompilerParams(vmem_limit_bytes=20 * 1024 * 1024),
        cost_estimate=pl.CostEstimate(flops=4_000_000_000, bytes_accessed=4_000_000, transcendentals=0),
        name="near_rows",
    )(state, raw, reach, gating, weight)


def project_kernel(partial, theirs, their_weight, final, out, final_out):
    out[...] = (partial[...] + mm(theirs[...], their_weight[...])).astype(BF16)
    final_out[...] = final[...]


def project(partial, theirs, their_weight, final, rows):
    total, width = partial.shape
    inner = theirs.shape[1]
    whole = pl.BlockSpec(final.shape, lambda i: (0, 0))
    return pl.pallas_call(
        project_kernel,
        grid=(total // rows,),
        in_specs=[
            pl.BlockSpec((rows, width), lambda i: (i, 0)),
            pl.BlockSpec((rows, inner), lambda i: (i, 0)),
            pl.BlockSpec((inner, width), lambda i: (0, 0)),
            whole,
        ],
        out_specs=[pl.BlockSpec((rows, width), lambda i: (i, 0)), whole],
        out_shape=[
            jax.ShapeDtypeStruct((total, width), BF16),
            jax.ShapeDtypeStruct(final.shape, F32),
        ],
        compiler_params=params(20),
        cost_estimate=pl.CostEstimate(flops=3_300_000_000, bytes_accessed=9_000_000, transcendentals=0),
        name="project",
    )(partial, theirs, pltpu.with_memory_space_constraint(their_weight, pltpu.VMEM), final)


def per_device(
    queries, forget_logit, value_rows, out_gate, floor_gap, head_gain, state_in, out_weight
):
    heads = state_in.shape[0]
    plane = lax.axis_size(PLANE)
    depth = lax.axis_size(Z)
    swap = [(0, 1), (1, 0)]
    barrier = lax.optimization_barrier
    gap = floor_gap.reshape(1, -1)
    gain = head_gain.reshape(1, -1)

    local, send, left = stretch(
        gap, gain, queries, forget_logit, value_rows, out_gate, heads, plane, depth, UNROLL
    )
    send, out_weight = barrier((send, out_weight))
    their_weight = lax.ppermute(out_weight, "tp", swap)
    received = lax.all_to_all(send, PLANE, 0, 0, tiled=True)

    send, prefix, product = plane_scan(received, heads, depth)
    received = lax.all_to_all(send, Z, 0, 0, tiled=True)
    send, final, *local = depth_scan(
        received, prefix, product, state_in, left, local, heads
    )
    incoming = lax.all_to_all(send, PLANE, 0, 0, tiled=True)

    far, state = far_rows(incoming, *local, heads, depth)
    theirs = lax.ppermute(far, "tp", swap)
    partial = near_rows(state, *local, out_weight, heads, 384)
    projected, state_out = project(partial, theirs, their_weight, final, 384)
    return (projected, state_out)


def solution(mesh):
    torus = Mesh(mesh.devices.reshape(8, 4, 4, mesh.shape["tp"]), (Z, Y, X, "tp"))
    placed = (
        P(SP, "tp"),
        P(SP, "tp"),
        P(SP, "tp"),
        P(SP, "tp"),
        P("tp"),
        P("tp"),
        P("tp", None, None),
        P("tp", None),
    )
    return jax.shard_map(
        per_device,
        mesh=torus,
        in_specs=placed,
        out_specs=(P(SP_TP, None), P("tp", SP)),
        check_vma=False,
    )
```

```python
import functools

import jax
import jax.numpy as jnp
from jax import lax
from jax.experimental import pallas as pl
from jax.experimental.pallas import tpu as pltpu
from jax.sharding import Mesh
from jax.sharding import PartitionSpec as P

BLOCK = 128
UNROLL = 4
EPSILON = 1e-06
LOG2E = 1.4426950408889634
Z, Y, X = ("sp_0", "sp_1", "sp_2")
SP = (Z, Y, X)
PLANE = (Y, X)
SP_TP = (Z, Y, X, "tp")
F32 = jnp.float32
BF16 = jnp.bfloat16


def mm(a, b, dims=((1,), (0,))):
    return lax.dot_general(a, b, (dims, ((), ())), preferred_element_type=F32)


def iota(shape, axis):
    return lax.broadcasted_iota(jnp.int32, shape, axis)


def params(limit_mib):
    return pltpu.CompilerParams(
        dimension_semantics=("arbitrary",), vmem_limit_bytes=limit_mib * 1024 * 1024
    )


def deal_matrix(plane, depth, transposed):
    rows = plane * depth
    dealt = iota((rows, rows), 1 if transposed else 0)
    natural = iota((rows, rows), 0 if transposed else 1)
    return ((dealt % depth) * plane + dealt // depth == natural).astype(BF16)


def log2_of_rest(gate):
    near = gate * (gate * (-LOG2E / 2) - LOG2E)
    return jnp.where(gate < 1e-3, near, jnp.log2(1.0 - gate))


def goes_early(depth):
    return lax.axis_index(Z) < depth * 3 // 8


def rows_of(block):
    return pl.ds(pl.multiple_of(block * BLOCK, BLOCK), BLOCK)


def read_block(rows, cols, query, gate, gain, cumul, offset, key, state):
    reader = jax.nn.silu(query[rows, cols].astype(F32)) * jnp.exp2(cumul)
    reach = (reader * offset).astype(BF16)
    both = mm(reader.astype(BF16), jnp.concatenate([key, state], axis=0), ((1,), (1,)))
    gating = jax.nn.silu(gate[rows, cols].astype(F32)) * gain[:, cols]
    return both, reach, gating


def finish_block(causal, both, values):
    scores = jnp.where(causal, both[:, :BLOCK], 0.0).astype(BF16)
    return mm(scores, values) + both[:, BLOCK:]


def stretch_kernel(heads, plane, depth, unroll, gap_in, gain_in, query_in, logit_in, value_in,
                   gate_in, raw_out, reach_out, gating_out, send_out, query, value, gate, cumuls,
                   keys, starts, offsets, gain, logit, key_gates, gap, state, decay, pair,
                   sems, small_sems):
    blocks = query.shape[0] // BLOCK
    sides = ((value_in, value), (query_in, query), (gate_in, gate))
    rest = [
        pltpu.make_async_copy(source, target, small_sems.at[2 + n])
        for n, (source, target) in enumerate(sides)
    ]

    def logits(i):
        rows = pl.ds(i * unroll * BLOCK, unroll * BLOCK)
        return pltpu.make_async_copy(logit_in.at[rows, :], logit.at[rows, :], sems.at[i])

    small = [
        pltpu.make_async_copy(gap_in, gap, small_sems.at[0]),
        pltpu.make_async_copy(gain_in, gain, small_sems.at[1]),
    ]
    logits(0).start()
    for copy in small:
        copy.start()
    for i in range(1, blocks // unroll):
        logits(i).start()
    for copy in rest:
        copy.start()
    state[...] = jnp.zeros_like(state)
    decay[...] = jnp.ones_like(decay)
    causal = iota((BLOCK, BLOCK), 0) >= iota((BLOCK, BLOCK), 1)
    lower = causal.astype(BF16)
    lower2 = jnp.concatenate([lower, lower], axis=1)
    head_cols = [pl.ds(h * 128, 128) for h in range(heads)]
    for copy in small:
        copy.wait()

    half_gap = 0.5 * gap[...]

    def sum_logs(i, carry):
        logits(i).wait()
        for b in range(unroll):
            rows = rows_of(i * unroll + b)
            highs, lows = [], []
            for h, cols in enumerate(head_cols):
                key_gate = half_gap[:, h * 128 : (h + 1) * 128] * (1.0 - jnp.tanh(0.5 * logit[rows, cols].astype(F32)))
                key_gates[rows, cols] = key_gate
                log_forget = log2_of_rest(key_gate)
                highs.append(log_forget.astype(BF16))
                lows.append((log_forget - highs[-1].astype(F32)).astype(BF16))
            split = jnp.concatenate(
                [jnp.concatenate(highs, axis=1), jnp.concatenate(lows, axis=1)], axis=0
            )
            cumuls[rows, :] = mm(lower2, split)
        return carry

    lax.fori_loop(0, blocks // unroll, sum_logs, 0)
    rest[0].wait()

    def advance(whole, i, carry):
        for b in range(unroll):
            block = i * unroll + b
            rows = rows_of(block)
            boths, updates, decays = [], [], []
            for cols in head_cols:
                cumul = cumuls[rows, cols]
                key = (key_gates[rows, cols] * jnp.exp2(-cumul)).astype(BF16)
                start = state[:, cols].astype(BF16)
                if whole:
                    both, reach_out[rows, cols], gating_out[rows, cols] = read_block(
                        rows, cols, query, gate, gain, cumul, decay[:, cols], key, start
                    )
                    boths.append(both)
                else:
                    keys[rows, cols] = key
                    starts[block, :, cols] = start
                    offsets[block, :, cols] = decay[:, cols]
                updates.append(mm(value[rows, cols], key, ((0,), (0,))))
                decays.append(jnp.exp2(cumul[BLOCK - 1 :, :]))
            for h, cols in enumerate(head_cols):
                if whole:
                    raw_out[rows, cols] = finish_block(causal, boths[h], value[rows, cols])
                state[:, cols] = decays[h] * (state[:, cols] + updates[h])
                decay[:, cols] = decay[:, cols] * decays[h]
        return carry

    early = goes_early(depth)

    @pl.when(early)
    def _():
        for copy in rest[1:]:
            copy.wait()
        lax.fori_loop(0, blocks // unroll, functools.partial(advance, True), 0)

    @pl.when(jnp.logical_not(early))
    def _():
        lax.fori_loop(0, blocks // unroll, functools.partial(advance, False), 0)
        for copy in rest[1:]:
            copy.wait()

    deal = deal_matrix(plane, depth, False)
    for h in range(heads):
        cols = pl.ds(h * 128, 128)
        dealt = mm(deal, state[:, cols].astype(BF16), ((1,), (1,)))
        send_out[:, h * depth : (h + 1) * depth, :] = (
            dealt.reshape(plane, depth, 128).astype(BF16)
        )
        whole = decay[:, cols]
        high = whole.astype(BF16).astype(F32)
        pair[h : h + 1, :] = high
        pair[heads + h : heads + h + 1, :] = whole - high
    tail = pair[...].astype(BF16)
    for p in range(plane):
        send_out[p, heads * depth :, :] = tail


def late_outputs(heads, query, value, gate, cumuls, keys, starts, offsets, gain,
                 raw_out, reach_out, gating_out):
    blocks = query.shape[0] // BLOCK
    causal = iota((BLOCK, BLOCK), 0) >= iota((BLOCK, BLOCK), 1)
    head_cols = [pl.ds(h * 128, 128) for h in range(heads)]

    def step(i, carry):
        for b in range(UNROLL):
            block = i * UNROLL + b
            rows = rows_of(block)
            boths = []
            for cols in head_cols:
                both, reach_out[rows, cols], gating_out[rows, cols] = read_block(
                    rows, cols, query, gate, gain, cumuls[rows, cols], offsets[block, :, cols],
                    keys[rows, cols], starts[block, :, cols],
                )
                boths.append(both)
            for both, cols in zip(boths, head_cols):
                raw_out[rows, cols] = finish_block(causal, both, value[rows, cols])
        return carry

    lax.fori_loop(0, blocks // UNROLL, step, 0)


VMEM_SPEC = pl.BlockSpec(memory_space=pltpu.VMEM)
HBM_SPEC = pl.BlockSpec(memory_space=pltpu.HBM)


def in_hbm(*arrays):
    return [pltpu.with_memory_space_constraint(array, pltpu.HBM) for array in arrays]


def stretch(gap, gain, query, logit, value, gate, heads, plane, depth, unroll):
    span, width = query.shape
    steps = span // BLOCK // unroll
    narrow = jax.ShapeDtypeStruct((span, width), BF16)
    wide = jax.ShapeDtypeStruct((span, width), F32)
    results = pl.pallas_call(
        functools.partial(stretch_kernel, heads, plane, depth, unroll),
        in_specs=[HBM_SPEC] * 6,
        out_specs=[VMEM_SPEC] * 12,
        out_shape=[
            wide,
            narrow,
            wide,
            jax.ShapeDtypeStruct((plane, heads * depth + 2 * heads, 128), BF16),
            narrow,
            narrow,
            narrow,
            wide,
            narrow,
            jax.ShapeDtypeStruct((span // BLOCK, 128, width), BF16),
            jax.ShapeDtypeStruct((span // BLOCK, 1, width), F32),
            jax.ShapeDtypeStruct((1, width), F32),
        ],
        scratch_shapes=[
            pltpu.VMEM((span, width), BF16),
            pltpu.VMEM((span, width), F32),
            pltpu.VMEM((1, width), F32),
            pltpu.VMEM((128, width), F32),
            pltpu.VMEM((1, width), F32),
            pltpu.VMEM((2 * heads, 128), F32),
            pltpu.SemaphoreType.DMA((steps,)),
            pltpu.SemaphoreType.DMA((5,)),
        ],
        compiler_params=pltpu.CompilerParams(vmem_limit_bytes=34 * 1024 * 1024),
        cost_estimate=pl.CostEstimate(flops=6_000_000_000, bytes_accessed=10_000_000, transcendentals=0),
        name="stretch",
    )(*in_hbm(gap, gain, query, logit, value, gate))
    return results[:3], results[3], results[4:]


def decay_columns(place, received, heads, depth, plane):
    count = received.shape[0]
    picked = (iota((depth, 128), 1) == iota((depth, 128), 0) * plane + place).astype(BF16)
    parts = received[:, heads * depth :, :].reshape(count * 2 * heads, 128)
    columns = mm(picked, parts, ((1,), (1,)))
    lanes = columns.shape[1]
    return columns + pltpu.roll(columns, lanes - heads, 1)


def plane_kernel(heads, plane, depth, received, send_out, prefix_out, product_out):
    columns = decay_columns(lax.axis_index(PLANE), received, heads, depth, plane)
    total = None
    states = [jnp.zeros((depth, 128), F32) for _ in range(heads)]
    products = [jnp.ones((depth, 128), F32) for _ in range(heads)]
    for s in range(plane):
        parts = received[s, heads * depth :, :].astype(F32)
        row_decay = parts + pltpu.roll(parts, heads, 0)
        total = row_decay if total is None else total * row_decay
        for h in range(heads):
            rows = slice(h * depth, (h + 1) * depth)
            prefix_out[s, rows, :] = states[h]
            product_out[s, rows, :] = products[h]
            lane = s * 2 * heads + h
            decay = jnp.broadcast_to(columns[:, lane : lane + 1], (depth, 128))
            states[h] = decay * states[h] + received[s, rows, :].astype(F32)
            products[h] = decay * products[h]
    high = total.astype(BF16).astype(F32)
    tail = jnp.where(iota(total.shape, 0) < heads, high, total - high).astype(BF16)
    for d in range(send_out.shape[0]):
        for h in range(heads):
            send_out[d, h * depth : (h + 1) * depth, :] = states[h].astype(BF16)
        send_out[d, heads * depth :, :] = tail


def plane_scan(received, heads, depth):
    plane, tall, _ = received.shape
    rows = heads * depth
    return pl.pallas_call(
        functools.partial(plane_kernel, heads, plane, depth),
        in_specs=[VMEM_SPEC],
        out_specs=[VMEM_SPEC] * 3,
        out_shape=[
            jax.ShapeDtypeStruct((depth, tall, 128), BF16),
            jax.ShapeDtypeStruct((plane, rows, 128), F32),
            jax.ShapeDtypeStruct((plane, rows, 128), F32),
        ],
        compiler_params=pltpu.CompilerParams(vmem_limit_bytes=8 * 1024 * 1024),
        cost_estimate=pl.CostEstimate(flops=100_000_000, bytes_accessed=1_000_000, transcendentals=0),
        name="plane_scan",
    )(received)


def depth_kernel(heads, plane, depth, received, prefix, product, first, query, value, gate,
                 cumuls, keys, starts, offsets, gain, raw_in, reach_in, gating_in,
                 send_out, final_out, raw_out, reach_out, gating_out, entering, final):
    columns = decay_columns(lax.axis_index(PLANE), received, heads, depth, plane)
    states = [first[h, pl.ds(lax.axis_index(PLANE), depth, stride=plane), :] for h in range(heads)]
    for s in range(depth):
        for h in range(heads):
            rows = slice(h * depth, (h + 1) * depth)
            entering[s, rows, :] = states[h]
            lane = s * 2 * heads + h
            decay = jnp.broadcast_to(columns[:, lane : lane + 1], (depth, 128))
            states[h] = decay * states[h] + received[s, rows, :].astype(F32)
    for h in range(heads):
        final[h] = states[h]
        final_out[h : h + 1, :] = final[h, pl.ds(lax.axis_index(Z), 1), :]
    mine = entering[lax.axis_index(Z)]
    for p in range(plane):
        send_out[p] = (prefix[p] + product[p] * mine).astype(BF16)

    @pl.when(jnp.logical_not(goes_early(depth)))
    def _():
        late_outputs(heads, query, value, gate, cumuls, keys, starts, offsets, gain,
                     raw_out, reach_out, gating_out)


def depth_scan(received, prefix, product, first, left, local, heads):
    depth, tall, _ = received.shape
    plane, rows, _ = prefix.shape
    return pl.pallas_call(
        functools.partial(depth_kernel, heads, plane, depth),
        in_specs=[VMEM_SPEC] * 15,
        out_specs=[VMEM_SPEC] * 5,
        out_shape=[
            jax.ShapeDtypeStruct((plane, rows, 128), BF16),
            jax.ShapeDtypeStruct((heads, 128), F32),
        ]
        + [jax.ShapeDtypeStruct(array.shape, array.dtype) for array in local],
        input_output_aliases={12: 2, 13: 3, 14: 4},
        scratch_shapes=[
            pltpu.VMEM((depth, rows, 128), F32),
            pltpu.VMEM((heads, depth, 128), F32),
        ],
        compiler_params=pltpu.CompilerParams(vmem_limit_bytes=30 * 1024 * 1024),
        cost_estimate=pl.CostEstimate(flops=100_000_000, bytes_accessed=1_000_000, transcendentals=0),
        name="depth_scan",
    )(received, prefix, product, first, *left, *local)


def gather_state(heads, depth, incoming, state):
    plane = incoming.shape[0]
    collect = deal_matrix(plane, depth, True)
    for h in range(heads):
        part = incoming[:, h * depth : (h + 1) * depth, :].astype(F32)
        part = part.reshape(plane * depth, 128).astype(BF16)
        state[h] = mm(collect, part).astype(BF16)


def gated_block(heads, source, raw, reach, gating, state, gated_out, target):
    rows = pl.ds(pl.multiple_of(source, BLOCK), BLOCK)
    for h in range(heads):
        cols = pl.ds(h * 128, 128)
        value = raw[rows, cols] + mm(reach[rows, cols], state[h])
        mean_square = jnp.mean(value * value, axis=-1, keepdims=True)
        gated_out[target : target + BLOCK, cols] = (
            value * lax.rsqrt(mean_square + EPSILON) * gating[rows, cols]
        ).astype(BF16)


def far_kernel(heads, depth, incoming, raw, reach, gating, gated_out, state):
    gather_state(heads, depth, incoming, state)
    half = gated_out.shape[0]
    first = (1 - lax.axis_index("tp")) * half
    for row in range(0, half, BLOCK):
        gated_block(heads, first + row, raw, reach, gating, state, gated_out, row)


def near_kernel(heads, tall, state, raw, reach, gating, weight, partial_out, gated):
    half = partial_out.shape[0]
    first = lax.axis_index("tp") * half
    for row in range(0, half, BLOCK):
        gated_block(heads, first + row, raw, reach, gating, state, gated, row)
        if (row + BLOCK) % tall == 0:
            done = pl.ds(row + BLOCK - tall, tall)
            partial_out[done, :] = mm(gated[done, :], weight[...])


def far_rows(incoming, raw, reach, gating, heads, depth):
    span, width = raw.shape
    return pl.pallas_call(
        functools.partial(far_kernel, heads, depth),
        in_specs=[VMEM_SPEC] * 4,
        out_specs=[VMEM_SPEC] * 2,
        out_shape=[
            jax.ShapeDtypeStruct((span // 2, width), BF16),
            jax.ShapeDtypeStruct((heads, 128, 128), BF16),
        ],
        compiler_params=pltpu.CompilerParams(vmem_limit_bytes=12 * 1024 * 1024),
        cost_estimate=pl.CostEstimate(flops=2_000_000_000, bytes_accessed=4_000_000, transcendentals=0),
        name="far_rows",
    )(incoming, raw, reach, gating)


def near_rows(state, raw, reach, gating, weight, heads, rows):
    span, width = raw.shape
    return pl.pallas_call(
        functools.partial(near_kernel, heads, rows),
        in_specs=[VMEM_SPEC] * 5,
        out_specs=VMEM_SPEC,
        out_shape=jax.ShapeDtypeStruct((span // 2, weight.shape[1]), F32),
        scratch_shapes=[pltpu.VMEM((span // 2, width), BF16)],
        compiler_params=pltpu.CompilerParams(vmem_limit_bytes=20 * 1024 * 1024),
        cost_estimate=pl.CostEstimate(flops=4_000_000_000, bytes_accessed=4_000_000, transcendentals=0),
        name="near_rows",
    )(state, raw, reach, gating, weight)


def project_kernel(partial, theirs, their_weight, final, out, final_out):
    out[...] = (partial[...] + mm(theirs[...], their_weight[...])).astype(BF16)
    final_out[...] = final[...]


def project(partial, theirs, their_weight, final, rows):
    total, width = partial.shape
    inner = theirs.shape[1]
    whole = pl.BlockSpec(final.shape, lambda i: (0, 0))
    return pl.pallas_call(
        project_kernel,
        grid=(total // rows,),
        in_specs=[
            pl.BlockSpec((rows, width), lambda i: (i, 0)),
            pl.BlockSpec((rows, inner), lambda i: (i, 0)),
            pl.BlockSpec((inner, width), lambda i: (0, 0)),
            whole,
        ],
        out_specs=[pl.BlockSpec((rows, width), lambda i: (i, 0)), whole],
        out_shape=[
            jax.ShapeDtypeStruct((total, width), BF16),
            jax.ShapeDtypeStruct(final.shape, F32),
        ],
        compiler_params=params(20),
        cost_estimate=pl.CostEstimate(flops=3_300_000_000, bytes_accessed=9_000_000, transcendentals=0),
        name="project",
    )(partial, theirs, pltpu.with_memory_space_constraint(their_weight, pltpu.VMEM), final)


def per_device(
    queries, forget_logit, value_rows, out_gate, floor_gap, head_gain, state_in, out_weight
):
    heads = state_in.shape[0]
    plane = lax.axis_size(PLANE)
    depth = lax.axis_size(Z)
    swap = [(0, 1), (1, 0)]
    barrier = lax.optimization_barrier
    gap = floor_gap.reshape(1, -1)
    gain = head_gain.reshape(1, -1)

    local, send, left = stretch(
        gap, gain, queries, forget_logit, value_rows, out_gate, heads, plane, depth, UNROLL
    )
    send, out_weight = barrier((send, out_weight))
    their_weight = lax.ppermute(out_weight, "tp", swap)
    received = lax.all_to_all(send, PLANE, 0, 0, tiled=True)

    send, prefix, product = plane_scan(received, heads, depth)
    received = lax.all_to_all(send, Z, 0, 0, tiled=True)
    send, final, *local = depth_scan(
        received, prefix, product, state_in, left, local, heads
    )
    incoming = lax.all_to_all(send, PLANE, 0, 0, tiled=True)

    far, state = far_rows(incoming, *local, heads, depth)
    theirs = lax.ppermute(far, "tp", swap)
    partial = near_rows(state, *local, out_weight, heads, 768)
    projected, state_out = project(partial, theirs, their_weight, final, 384)
    return (projected, state_out)


def solution(mesh):
    torus = Mesh(mesh.devices.reshape(8, 4, 4, mesh.shape["tp"]), (Z, Y, X, "tp"))
    placed = (
        P(SP, "tp"),
        P(SP, "tp"),
        P(SP, "tp"),
        P(SP, "tp"),
        P("tp"),
        P("tp"),
        P("tp", None, None),
        P("tp", None),
    )
    return jax.shard_map(
        per_device,
        mesh=torus,
        in_specs=placed,
        out_specs=(P(SP_TP, None), P("tp", SP)),
        check_vma=False,
    )
```

```python
import functools

import jax
import jax.numpy as jnp
from jax import lax
from jax.experimental import pallas as pl
from jax.experimental.pallas import tpu as pltpu
from jax.sharding import Mesh
from jax.sharding import PartitionSpec as P

BLOCK = 128
UNROLL = 4
EPSILON = 1e-06
LOG2E = 1.4426950408889634
Z, Y, X = ("sp_0", "sp_1", "sp_2")
SP = (Z, Y, X)
PLANE = (Y, X)
SP_TP = (Z, Y, X, "tp")
F32 = jnp.float32
BF16 = jnp.bfloat16


def mm(a, b, dims=((1,), (0,))):
    return lax.dot_general(a, b, (dims, ((), ())), preferred_element_type=F32)


def iota(shape, axis):
    return lax.broadcasted_iota(jnp.int32, shape, axis)


def params(limit_mib):
    return pltpu.CompilerParams(
        dimension_semantics=("arbitrary",), vmem_limit_bytes=limit_mib * 1024 * 1024
    )


def deal_matrix(plane, depth, transposed):
    rows = plane * depth
    dealt = iota((rows, rows), 1 if transposed else 0)
    natural = iota((rows, rows), 0 if transposed else 1)
    return ((dealt % depth) * plane + dealt // depth == natural).astype(BF16)


def log2_of_rest(gate):
    near = gate * (gate * (-LOG2E / 2) - LOG2E)
    return jnp.where(gate < 1e-3, near, jnp.log2(1.0 - gate))


def goes_early(depth):
    return lax.axis_index(Z) < depth // 4


def rows_of(block):
    return pl.ds(pl.multiple_of(block * BLOCK, BLOCK), BLOCK)


def read_block(rows, cols, query, gate, gain, cumul, offset, key, state):
    reader = jax.nn.silu(query[rows, cols].astype(F32)) * jnp.exp2(cumul)
    reach = (reader * offset).astype(BF16)
    both = mm(reader.astype(BF16), jnp.concatenate([key, state], axis=0), ((1,), (1,)))
    gating = jax.nn.silu(gate[rows, cols].astype(F32)) * gain[:, cols]
    return both, reach, gating


def finish_block(causal, both, values):
    scores = jnp.where(causal, both[:, :BLOCK], 0.0).astype(BF16)
    return mm(scores, values) + both[:, BLOCK:]


def stretch_kernel(heads, plane, depth, unroll, gap_in, gain_in, query_in, logit_in, value_in,
                   gate_in, raw_out, reach_out, gating_out, send_out, query, value, gate, cumuls,
                   keys, starts, offsets, gain, logit, key_gates, gap, state, decay, pair,
                   sems, small_sems):
    blocks = query.shape[0] // BLOCK
    sides = ((value_in, value), (query_in, query), (gate_in, gate))
    rest = [
        pltpu.make_async_copy(source, target, small_sems.at[2 + n])
        for n, (source, target) in enumerate(sides)
    ]

    def logits(i):
        rows = pl.ds(i * unroll * BLOCK, unroll * BLOCK)
        return pltpu.make_async_copy(logit_in.at[rows, :], logit.at[rows, :], sems.at[i])

    small = [
        pltpu.make_async_copy(gap_in, gap, small_sems.at[0]),
        pltpu.make_async_copy(gain_in, gain, small_sems.at[1]),
    ]
    logits(0).start()
    for copy in small:
        copy.start()
    for i in range(1, blocks // unroll):
        logits(i).start()
    for copy in rest:
        copy.start()
    state[...] = jnp.zeros_like(state)
    decay[...] = jnp.ones_like(decay)
    causal = iota((BLOCK, BLOCK), 0) >= iota((BLOCK, BLOCK), 1)
    lower = causal.astype(BF16)
    lower2 = jnp.concatenate([lower, lower], axis=1)
    head_cols = [pl.ds(h * 128, 128) for h in range(heads)]
    for copy in small:
        copy.wait()

    half_gap = 0.5 * gap[...]

    def sum_logs(i, carry):
        logits(i).wait()
        for b in range(unroll):
            rows = rows_of(i * unroll + b)
            highs, lows = [], []
            for h, cols in enumerate(head_cols):
                key_gate = half_gap[:, h * 128 : (h + 1) * 128] * (1.0 - jnp.tanh(0.5 * logit[rows, cols].astype(F32)))
                key_gates[rows, cols] = key_gate
                log_forget = log2_of_rest(key_gate)
                highs.append(log_forget.astype(BF16))
                lows.append((log_forget - highs[-1].astype(F32)).astype(BF16))
            split = jnp.concatenate(
                [jnp.concatenate(highs, axis=1), jnp.concatenate(lows, axis=1)], axis=0
            )
            cumuls[rows, :] = mm(lower2, split)
        return carry

    lax.fori_loop(0, blocks // unroll, sum_logs, 0)
    rest[0].wait()

    def advance(whole, i, carry):
        for b in range(unroll):
            block = i * unroll + b
            rows = rows_of(block)
            boths, updates, decays = [], [], []
            for cols in head_cols:
                cumul = cumuls[rows, cols]
                key = (key_gates[rows, cols] * jnp.exp2(-cumul)).astype(BF16)
                start = state[:, cols].astype(BF16)
                if whole:
                    both, reach_out[rows, cols], gating_out[rows, cols] = read_block(
                        rows, cols, query, gate, gain, cumul, decay[:, cols], key, start
                    )
                    boths.append(both)
                else:
                    keys[rows, cols] = key
                    starts[block, :, cols] = start
                    offsets[block, :, cols] = decay[:, cols]
                updates.append(mm(value[rows, cols], key, ((0,), (0,))))
                decays.append(jnp.exp2(cumul[BLOCK - 1 :, :]))
            for h, cols in enumerate(head_cols):
                if whole:
                    raw_out[rows, cols] = finish_block(causal, boths[h], value[rows, cols])
                state[:, cols] = decays[h] * (state[:, cols] + updates[h])
                decay[:, cols] = decay[:, cols] * decays[h]
        return carry

    early = goes_early(depth)

    @pl.when(early)
    def _():
        for copy in rest[1:]:
            copy.wait()
        lax.fori_loop(0, blocks // unroll, functools.partial(advance, True), 0)

    @pl.when(jnp.logical_not(early))
    def _():
        lax.fori_loop(0, blocks // unroll, functools.partial(advance, False), 0)
        for copy in rest[1:]:
            copy.wait()

    deal = deal_matrix(plane, depth, False)
    for h in range(heads):
        cols = pl.ds(h * 128, 128)
        dealt = mm(deal, state[:, cols].astype(BF16), ((1,), (1,)))
        send_out[:, h * depth : (h + 1) * depth, :] = (
            dealt.reshape(plane, depth, 128).astype(BF16)
        )
        whole = decay[:, cols]
        high = whole.astype(BF16).astype(F32)
        pair[h : h + 1, :] = high
        pair[heads + h : heads + h + 1, :] = whole - high
    tail = pair[...].astype(BF16)
    for p in range(plane):
        send_out[p, heads * depth :, :] = tail


def late_outputs(heads, query, value, gate, cumuls, keys, starts, offsets, gain,
                 raw_out, reach_out, gating_out):
    blocks = query.shape[0] // BLOCK
    causal = iota((BLOCK, BLOCK), 0) >= iota((BLOCK, BLOCK), 1)
    head_cols = [pl.ds(h * 128, 128) for h in range(heads)]

    def step(i, carry):
        for b in range(UNROLL):
            block = i * UNROLL + b
            rows = rows_of(block)
            boths = []
            for cols in head_cols:
                both, reach_out[rows, cols], gating_out[rows, cols] = read_block(
                    rows, cols, query, gate, gain, cumuls[rows, cols], offsets[block, :, cols],
                    keys[rows, cols], starts[block, :, cols],
                )
                boths.append(both)
            for both, cols in zip(boths, head_cols):
                raw_out[rows, cols] = finish_block(causal, both, value[rows, cols])
        return carry

    lax.fori_loop(0, blocks // UNROLL, step, 0)


VMEM_SPEC = pl.BlockSpec(memory_space=pltpu.VMEM)
HBM_SPEC = pl.BlockSpec(memory_space=pltpu.HBM)


def in_hbm(*arrays):
    return [pltpu.with_memory_space_constraint(array, pltpu.HBM) for array in arrays]


def stretch(gap, gain, query, logit, value, gate, heads, plane, depth, unroll):
    span, width = query.shape
    steps = span // BLOCK // unroll
    narrow = jax.ShapeDtypeStruct((span, width), BF16)
    wide = jax.ShapeDtypeStruct((span, width), F32)
    results = pl.pallas_call(
        functools.partial(stretch_kernel, heads, plane, depth, unroll),
        in_specs=[HBM_SPEC] * 6,
        out_specs=[VMEM_SPEC] * 12,
        out_shape=[
            wide,
            narrow,
            wide,
            jax.ShapeDtypeStruct((plane, heads * depth + 2 * heads, 128), BF16),
            narrow,
            narrow,
            narrow,
            wide,
            narrow,
            jax.ShapeDtypeStruct((span // BLOCK, 128, width), BF16),
            jax.ShapeDtypeStruct((span // BLOCK, 1, width), F32),
            jax.ShapeDtypeStruct((1, width), F32),
        ],
        scratch_shapes=[
            pltpu.VMEM((span, width), BF16),
            pltpu.VMEM((span, width), F32),
            pltpu.VMEM((1, width), F32),
            pltpu.VMEM((128, width), F32),
            pltpu.VMEM((1, width), F32),
            pltpu.VMEM((2 * heads, 128), F32),
            pltpu.SemaphoreType.DMA((steps,)),
            pltpu.SemaphoreType.DMA((5,)),
        ],
        compiler_params=pltpu.CompilerParams(vmem_limit_bytes=34 * 1024 * 1024),
        cost_estimate=pl.CostEstimate(flops=6_000_000_000, bytes_accessed=10_000_000, transcendentals=0),
        name="stretch",
    )(*in_hbm(gap, gain, query, logit, value, gate))
    return results[:3], results[3], results[4:]


def decay_columns(place, received, heads, depth, plane):
    count = received.shape[0]
    picked = (iota((depth, 128), 1) == iota((depth, 128), 0) * plane + place).astype(BF16)
    parts = received[:, heads * depth :, :].reshape(count * 2 * heads, 128)
    columns = mm(picked, parts, ((1,), (1,)))
    lanes = columns.shape[1]
    return columns + pltpu.roll(columns, lanes - heads, 1)


def plane_kernel(heads, plane, depth, received, send_out, prefix_out, product_out):
    columns = decay_columns(lax.axis_index(PLANE), received, heads, depth, plane)
    total = None
    states = [jnp.zeros((depth, 128), F32) for _ in range(heads)]
    products = [jnp.ones((depth, 128), F32) for _ in range(heads)]
    for s in range(plane):
        parts = received[s, heads * depth :, :].astype(F32)
        row_decay = parts + pltpu.roll(parts, heads, 0)
        total = row_decay if total is None else total * row_decay
        for h in range(heads):
            rows = slice(h * depth, (h + 1) * depth)
            prefix_out[s, rows, :] = states[h]
            product_out[s, rows, :] = products[h]
            lane = s * 2 * heads + h
            decay = jnp.broadcast_to(columns[:, lane : lane + 1], (depth, 128))
            states[h] = decay * states[h] + received[s, rows, :].astype(F32)
            products[h] = decay * products[h]
    high = total.astype(BF16).astype(F32)
    tail = jnp.where(iota(total.shape, 0) < heads, high, total - high).astype(BF16)
    for d in range(send_out.shape[0]):
        for h in range(heads):
            send_out[d, h * depth : (h + 1) * depth, :] = states[h].astype(BF16)
        send_out[d, heads * depth :, :] = tail


def plane_scan(received, heads, depth):
    plane, tall, _ = received.shape
    rows = heads * depth
    return pl.pallas_call(
        functools.partial(plane_kernel, heads, plane, depth),
        in_specs=[VMEM_SPEC],
        out_specs=[VMEM_SPEC] * 3,
        out_shape=[
            jax.ShapeDtypeStruct((depth, tall, 128), BF16),
            jax.ShapeDtypeStruct((plane, rows, 128), F32),
            jax.ShapeDtypeStruct((plane, rows, 128), F32),
        ],
        compiler_params=pltpu.CompilerParams(vmem_limit_bytes=8 * 1024 * 1024),
        cost_estimate=pl.CostEstimate(flops=100_000_000, bytes_accessed=1_000_000, transcendentals=0),
        name="plane_scan",
    )(received)


def depth_kernel(heads, plane, depth, received, prefix, product, first, query, value, gate,
                 cumuls, keys, starts, offsets, gain, raw_in, reach_in, gating_in,
                 send_out, final_out, raw_out, reach_out, gating_out, entering, final):
    columns = decay_columns(lax.axis_index(PLANE), received, heads, depth, plane)
    states = [first[h, pl.ds(lax.axis_index(PLANE), depth, stride=plane), :] for h in range(heads)]
    for s in range(depth):
        for h in range(heads):
            rows = slice(h * depth, (h + 1) * depth)
            entering[s, rows, :] = states[h]
            lane = s * 2 * heads + h
            decay = jnp.broadcast_to(columns[:, lane : lane + 1], (depth, 128))
            states[h] = decay * states[h] + received[s, rows, :].astype(F32)
    for h in range(heads):
        final[h] = states[h]
        final_out[h : h + 1, :] = final[h, pl.ds(lax.axis_index(Z), 1), :]
    mine = entering[lax.axis_index(Z)]
    for p in range(plane):
        send_out[p] = (prefix[p] + product[p] * mine).astype(BF16)

    @pl.when(jnp.logical_not(goes_early(depth)))
    def _():
        late_outputs(heads, query, value, gate, cumuls, keys, starts, offsets, gain,
                     raw_out, reach_out, gating_out)


def depth_scan(received, prefix, product, first, left, local, heads):
    depth, tall, _ = received.shape
    plane, rows, _ = prefix.shape
    return pl.pallas_call(
        functools.partial(depth_kernel, heads, plane, depth),
        in_specs=[VMEM_SPEC] * 15,
        out_specs=[VMEM_SPEC] * 5,
        out_shape=[
            jax.ShapeDtypeStruct((plane, rows, 128), BF16),
            jax.ShapeDtypeStruct((heads, 128), F32),
        ]
        + [jax.ShapeDtypeStruct(array.shape, array.dtype) for array in local],
        input_output_aliases={12: 2, 13: 3, 14: 4},
        scratch_shapes=[
            pltpu.VMEM((depth, rows, 128), F32),
            pltpu.VMEM((heads, depth, 128), F32),
        ],
        compiler_params=pltpu.CompilerParams(vmem_limit_bytes=30 * 1024 * 1024),
        cost_estimate=pl.CostEstimate(flops=100_000_000, bytes_accessed=1_000_000, transcendentals=0),
        name="depth_scan",
    )(received, prefix, product, first, *left, *local)


def gather_state(heads, depth, incoming, state):
    plane = incoming.shape[0]
    collect = deal_matrix(plane, depth, True)
    for h in range(heads):
        part = incoming[:, h * depth : (h + 1) * depth, :].astype(F32)
        part = part.reshape(plane * depth, 128).astype(BF16)
        state[h] = mm(collect, part).astype(BF16)


def gated_block(heads, source, raw, reach, gating, state, gated_out, target):
    rows = pl.ds(pl.multiple_of(source, BLOCK), BLOCK)
    for h in range(heads):
        cols = pl.ds(h * 128, 128)
        value = raw[rows, cols] + mm(reach[rows, cols], state[h])
        mean_square = jnp.mean(value * value, axis=-1, keepdims=True)
        gated_out[target : target + BLOCK, cols] = (
            value * lax.rsqrt(mean_square + EPSILON) * gating[rows, cols]
        ).astype(BF16)


def far_kernel(heads, depth, incoming, raw, reach, gating, gated_out, state):
    gather_state(heads, depth, incoming, state)
    half = gated_out.shape[0]
    first = (1 - lax.axis_index("tp")) * half
    for row in range(0, half, BLOCK):
        gated_block(heads, first + row, raw, reach, gating, state, gated_out, row)


def near_kernel(heads, tall, state, raw, reach, gating, weight, partial_out, gated):
    half = partial_out.shape[0]
    first = lax.axis_index("tp") * half
    for row in range(0, half, BLOCK):
        gated_block(heads, first + row, raw, reach, gating, state, gated, row)
        if (row + BLOCK) % tall == 0:
            done = pl.ds(row + BLOCK - tall, tall)
            partial_out[done, :] = mm(gated[done, :], weight[...])


def far_rows(incoming, raw, reach, gating, heads, depth):
    span, width = raw.shape
    return pl.pallas_call(
        functools.partial(far_kernel, heads, depth),
        in_specs=[VMEM_SPEC] * 4,
        out_specs=[VMEM_SPEC] * 2,
        out_shape=[
            jax.ShapeDtypeStruct((span // 2, width), BF16),
            jax.ShapeDtypeStruct((heads, 128, 128), BF16),
        ],
        compiler_params=pltpu.CompilerParams(vmem_limit_bytes=12 * 1024 * 1024),
        cost_estimate=pl.CostEstimate(flops=2_000_000_000, bytes_accessed=4_000_000, transcendentals=0),
        name="far_rows",
    )(incoming, raw, reach, gating)


def near_rows(state, raw, reach, gating, weight, heads, rows):
    span, width = raw.shape
    return pl.pallas_call(
        functools.partial(near_kernel, heads, rows),
        in_specs=[VMEM_SPEC] * 5,
        out_specs=VMEM_SPEC,
        out_shape=jax.ShapeDtypeStruct((span // 2, weight.shape[1]), F32),
        scratch_shapes=[pltpu.VMEM((span // 2, width), BF16)],
        compiler_params=pltpu.CompilerParams(vmem_limit_bytes=20 * 1024 * 1024),
        cost_estimate=pl.CostEstimate(flops=4_000_000_000, bytes_accessed=4_000_000, transcendentals=0),
        name="near_rows",
    )(state, raw, reach, gating, weight)


def project_kernel(partial, theirs, their_weight, final, out, final_out):
    out[...] = (partial[...] + mm(theirs[...], their_weight[...])).astype(BF16)
    final_out[...] = final[...]


def project(partial, theirs, their_weight, final, rows):
    total, width = partial.shape
    inner = theirs.shape[1]
    whole = pl.BlockSpec(final.shape, lambda i: (0, 0))
    return pl.pallas_call(
        project_kernel,
        grid=(total // rows,),
        in_specs=[
            pl.BlockSpec((rows, width), lambda i: (i, 0)),
            pl.BlockSpec((rows, inner), lambda i: (i, 0)),
            pl.BlockSpec((inner, width), lambda i: (0, 0)),
            whole,
        ],
        out_specs=[pl.BlockSpec((rows, width), lambda i: (i, 0)), whole],
        out_shape=[
            jax.ShapeDtypeStruct((total, width), BF16),
            jax.ShapeDtypeStruct(final.shape, F32),
        ],
        compiler_params=params(20),
        cost_estimate=pl.CostEstimate(flops=3_300_000_000, bytes_accessed=9_000_000, transcendentals=0),
        name="project",
    )(partial, theirs, pltpu.with_memory_space_constraint(their_weight, pltpu.VMEM), final)


def per_device(
    queries, forget_logit, value_rows, out_gate, floor_gap, head_gain, state_in, out_weight
):
    heads = state_in.shape[0]
    plane = lax.axis_size(PLANE)
    depth = lax.axis_size(Z)
    swap = [(0, 1), (1, 0)]
    barrier = lax.optimization_barrier
    gap = floor_gap.reshape(1, -1)
    gain = head_gain.reshape(1, -1)

    local, send, left = stretch(
        gap, gain, queries, forget_logit, value_rows, out_gate, heads, plane, depth, UNROLL
    )
    send, out_weight = barrier((send, out_weight))
    their_weight = lax.ppermute(out_weight, "tp", swap)
    received = lax.all_to_all(send, PLANE, 0, 0, tiled=True)

    send, prefix, product = plane_scan(received, heads, depth)
    received = lax.all_to_all(send, Z, 0, 0, tiled=True)
    send, final, *local = depth_scan(
        received, prefix, product, state_in, left, local, heads
    )
    incoming = lax.all_to_all(send, PLANE, 0, 0, tiled=True)

    far, state = far_rows(incoming, *local, heads, depth)
    theirs = lax.ppermute(far, "tp", swap)
    partial = near_rows(state, *local, out_weight, heads, 768)
    projected, state_out = project(partial, theirs, their_weight, final, 384)
    return (projected, state_out)


def solution(mesh):
    torus = Mesh(mesh.devices.reshape(8, 4, 4, mesh.shape["tp"]), (Z, Y, X, "tp"))
    placed = (
        P(SP, "tp"),
        P(SP, "tp"),
        P(SP, "tp"),
        P(SP, "tp"),
        P("tp"),
        P("tp"),
        P("tp", None, None),
        P("tp", None),
    )
    return jax.shard_map(
        per_device,
        mesh=torus,
        in_specs=placed,
        out_specs=(P(SP_TP, None), P("tp", SP)),
        check_vma=False,
    )
```
